256 devices in a mesh: grp: 2 (over y), sp: 16 (over z), tp: 8 (over x, core).
Axes of the slice: x: 4, y: 2, z: 16, core: 2. Of those that a mesh axis runs over, the one named last changes fastest.
The devices are a block of a 4x16x16 slice.
Arguments:
- hidden_in: bfloat16 [12288, 4096], P(('grp', 'sp'), 'tp'), parts along dimension 0, may hold values from -30 to 30
- in_gain: float32 [2, 4096], P(None, 'tp'), may hold values from 0.1 to 1.9
- w_value: bfloat16 [2, 4096, 2048], P(None, 'sp', 'tp'), may hold values from -0.09375 to 0.09375
- w_gate: bfloat16 [2, 4096, 2048], P(None, 'sp', 'tp'), may hold values from -0.09375 to 0.09375
- conv_taps: float32 [2, 31, 2048], P(None, None, 'tp'), may hold values from -9 to 9
- norm_gain: float32 [2, 2048], P(None, 'tp'), may hold values from 0.1 to 1.9
- norm_shift: float32 [2, 2048], P(None, 'tp'), may hold values from -3 to 3
- w_out: bfloat16 [2, 2048, 4096], P(None, 'tp', 'sp'), may hold values from -0.125 to 0.125
Outputs:
- hidden_out: bfloat16 [12288, 4096], P(('grp', 'sp'), 'tp'), parts along dimension 0
The draws below stay inside these ranges and needn't reach their ends.
There are 2 independent parts, one for each index of `grp`. The reference program is written for one: setup_inputs(seed, part) draws one part's arguments, and reference() takes and returns one part's arrays. A program takes and returns all parts, laid end to end along the dimension named above; an argument that names none is the same for every part. Nothing has to cross between parts.
All inputs are finite; a program needn't handle non-finite values.
Results may differ from the reference program's by a relative error of at most 0.013.
Values may be sent and summed in bfloat16 or wider, within the bound.
A program may use at most 64 MiB of HBM per device.

```python
import math
import jax
import jax.numpy as jnp
from jax import lax

D = 4096
C = 2048
KERNEL = 31
LAYERS = 2
TOKENS = 6144
N_TP = 8


def draw_hidden_in(key, part):
    keys = jax.random.split(key, 3)
    base = jnp.clip(jax.random.normal(keys[0], (TOKENS, D), jnp.float32), -4.0, 4.0)
    ramp = 3.0 ** (jnp.arange(D, dtype=jnp.float32) / D - 0.5)
    column = ramp * jnp.exp(jax.random.uniform(keys[1], (D,), jnp.float32, math.log(0.6), math.log(1.6)))
    row_scale = jnp.exp(jax.random.uniform(keys[2], (TOKENS,), jnp.float32, math.log(0.4), math.log(2.5)))
    return (base * row_scale[:, None] * column[None, :]).astype(jnp.bfloat16)


def draw_conv_taps(key, part):
    keys = jax.random.split(key, 2)
    base = jnp.clip(jax.random.normal(keys[0], (LAYERS, KERNEL, C), jnp.float32), -4.0, 4.0)
    ramp = 3.0 ** (jnp.arange(C, dtype=jnp.float32) / C)
    channel = ramp * jnp.exp(jax.random.uniform(keys[1], (C,), jnp.float32, 0.0, math.log(4.0)))
    return base / math.sqrt(KERNEL) * channel[None, None, :]


def block_levels(own_key, extent, pieces, smallest, largest):
    level, own = 1.0, jax.random.fold_in(own_key, 6)
    for axis_at, parts in pieces:
        heights = jnp.exp(jax.random.uniform(jax.random.fold_in(own, axis_at), (parts,), jnp.float32, smallest / len(pieces), largest / len(pieces)))
        level = level * jnp.repeat(heights, extent[axis_at] // parts).reshape([-1 if axis == axis_at else 1 for axis in range(len(extent))])
    return level


def scatter_about(own_key, shape, spread, most, cuts=(), kind=jnp.bfloat16):
    drawn = spread * jax.random.normal(own_key, shape, jnp.float32)
    if cuts:
        drawn = drawn * block_levels(own_key, shape, cuts, -0.22, 0.18)
    return jnp.clip(drawn, -most, most).astype(kind)


def setup_inputs(seed: int = 0, part: int = 0) -> dict:
    key_of = jax.random.split(jax.random.key(seed), 9)
    own_keys = jax.random.split(jax.random.fold_in(key_of[8], part), 9)
    return {
        "hidden_in": draw_hidden_in(jax.random.fold_in(jax.random.fold_in(key_of[8], part), 71), part),
        "in_gain": jnp.clip(1.0 + 0.18 * jax.random.normal(key_of[1], (LAYERS, D), jnp.float32), 0.1, 1.9),
        "w_value": scatter_about(key_of[2], (LAYERS, D, C), D ** -0.5, 0.09375, ((1, 16), (2, 8))),
        "w_gate": scatter_about(key_of[3], (LAYERS, D, C), D ** -0.5, 0.09375, ((1, 16), (2, 8))),
        "conv_taps": draw_conv_taps(jax.random.fold_in(key_of[8], 71), part),
        "norm_gain": jnp.clip(1.0 + 0.18 * jax.random.normal(key_of[5], (LAYERS, C), jnp.float32), 0.1, 1.9),
        "norm_shift": scatter_about(key_of[6], (LAYERS, C), 0.5, 3.0, ((1, 8),), jnp.float32),
        "w_out": scatter_about(key_of[7], (LAYERS, C, D), C ** -0.5, 0.125, ((1, 8), (2, 16))),
    }


epsilon = 1e-06

def block_sum(mixed_out, weight):
    block_width = C // N_TP

    def add_block(block_index, running):
        offset = block_index.astype(jnp.int32) * block_width
        block_cols = lax.dynamic_slice_in_dim(mixed_out, offset, block_width, 1)
        block_rows = lax.dynamic_slice_in_dim(weight, offset, block_width, 0)
        partial_value = jnp.dot(block_cols, block_rows, preferred_element_type=jnp.float32).astype(jnp.bfloat16)
        partial_value = lax.optimization_barrier(partial_value)
        return running + partial_value.astype(jnp.float32)
    start_sum = jnp.zeros((mixed_out.shape[0], weight.shape[1]), jnp.float32)
    return lax.fori_loop(0, N_TP, add_block, start_sum)

def causal_taps(gated_wide, taps):
    row_total = gated_wide.shape[0]
    padded = jnp.concatenate([jnp.zeros((KERNEL - 1, gated_wide.shape[1]), jnp.float32), gated_wide], axis=0)

    def add_tap(tap_index, running):
        where = tap_index.astype(jnp.int32)
        window = lax.dynamic_slice_in_dim(padded, where, row_total, 0)
        weight_row = lax.dynamic_slice_in_dim(taps, where, 1, 0)
        return running + weight_row * window
    start_sum = jnp.zeros(gated_wide.shape, jnp.float32)
    return lax.fori_loop(0, KERNEL, add_tap, start_sum)

def reference(hidden_in, in_gain, w_value, w_gate, conv_taps, norm_gain, norm_shift, w_out):
    hidden = hidden_in
    for layer_idx in range(LAYERS):
        widened = hidden.astype(jnp.float32)
        inv_rms = lax.rsqrt(lax.optimization_barrier(jnp.mean(widened * widened, axis=1, keepdims=True)) + epsilon)
        normalized = (widened * inv_rms * in_gain[layer_idx]).astype(jnp.bfloat16)
        value_part = jnp.dot(normalized, w_value[layer_idx], preferred_element_type=jnp.float32)
        gate_part = jnp.dot(normalized, w_gate[layer_idx], preferred_element_type=jnp.float32)
        gated = (value_part * jax.nn.sigmoid(gate_part)).astype(jnp.bfloat16)
        conved = causal_taps(gated.astype(jnp.float32), conv_taps[layer_idx])
        row_mean = lax.optimization_barrier(jnp.mean(conved, axis=1, keepdims=True))
        variance = lax.optimization_barrier(jnp.mean(jnp.square(conved - row_mean), axis=1, keepdims=True))
        normed = (conved - row_mean) * lax.rsqrt(variance + epsilon) * norm_gain[layer_idx] + norm_shift[layer_idx]
        mixed_out = jax.nn.silu(normed).astype(jnp.bfloat16)
        branch = block_sum(mixed_out, w_out[layer_idx])
        hidden = (hidden.astype(jnp.float32) + branch).astype(jnp.bfloat16)
    return hidden
```

```python
import functools

import jax
import jax.numpy as jnp
from jax import lax
from jax.experimental import pallas as pl
from jax.experimental.pallas import tpu as pltpu
from jax.sharding import PartitionSpec as P

MESH = pl.DeviceIdType.MESH
EPS = 1e-06
F32 = jnp.float32
BF16 = jnp.bfloat16
RIGHT, LEFT = 1, -1


def mm(a, b):
    return jnp.dot(a, b, preferred_element_type=F32)


def both(col):
    return jnp.concatenate([col, col], axis=1)


def kernel(
    sizes,
    hidden,
    in_gain,
    w_value,
    w_gate,
    taps,
    norm_gain,
    norm_shift,
    w_out,
    out,
    wbuf,
    xg,
    cur,
    acc_v,
    acc_g,
    col_a,
    col_b,
    rstat,
    cstat,
    halo_out,
    halo_in,
    ext,
    shifted,
    conved,
    mixed,
    p_out,
    p_in,
    c_out,
    c_in,
    local_sem,
    z_send,
    z_recv,
    y_send,
    y_recv,
    x_send,
    x_recv,
    s_send,
    s_recv,
    h_send,
    h_recv,
    p_send,
    p_recv,
    c_send,
    c_recv,
):
    groups, ns, nt = sizes
    layers = w_value.shape[0]
    rows_w, ch = w_value.shape[1], w_value.shape[2]
    tokens = hidden.shape[0]
    n_taps = taps.shape[1]
    nx = nt // 2
    half = ns // 2
    channels = ch * nt
    features = hidden.shape[1] * nt
    z = lax.axis_index("sp")
    t = lax.axis_index("tp")
    paired = groups % 2 == 0
    x, c = t // 2, lax.rem(t, 2)

    def chip(dx, core):
        return 2 * lax.rem(x + dx + nx, nx) + core

    t_right, t_left, t_opp, t_mate = chip(1, c), chip(-1, c), chip(2, c), 2 * x + (1 - c)

    if paired:
        y = lax.axis_index("grp")
        par = lax.rem(y, 2)
        y_mate = y + 1 - 2 * par
        lone = 80
        ring_rows = rows_w - lone
        ring_at = pl.ds(pl.multiple_of(par * lone, 16), ring_rows)
        y_out_at = pl.ds(pl.multiple_of(par * ring_rows, 16), lone)
        y_in_at = pl.ds(pl.multiple_of((1 - par) * ring_rows, 16), lone)
    else:
        ring_at = pl.ds(0, rows_w)

    def zc(offset):
        return lax.rem(z + offset + 2 * ns, ns)

    def remote(src, dst, ssem, rsem, **where):
        return pltpu.make_async_remote_copy(
            src_ref=src, dst_ref=dst, send_sem=ssem, recv_sem=rsem, device_id=where, device_id_type=MESH
        )

    def z_copy(l, sub, d, s):
        at = wbuf.at[l, zc(-d * (s - 1)), sub, ring_at, :]
        way = 0 if d == RIGHT else 1
        return remote(at, at, z_send.at[l, sub, way, s % 2], z_recv.at[l, sub, way, s - 1], sp=zc(d))

    def z_arrival(l, sub, d, s):
        at = wbuf.at[l, zc(-d * s), sub, ring_at, :]
        way = 0 if d == RIGHT else 1
        return remote(at, at, z_send.at[l, sub, way, s % 2], z_recv.at[l, sub, way, s - 1], sp=zc(d))

    def active(l, sub, d, s):
        if s < half:
            return True
        return s == half and d == (RIGHT, LEFT, RIGHT if l % 2 == 0 else LEFT)[sub]

    def y_copy(l, chunk, slot, rows):
        at = wbuf.at[l, chunk, :, rows, :]
        return remote(at, at, y_send.at[l, slot], y_recv.at[l, slot], grp=y_mate)

    def hop_chunks(s):
        if s == 0:
            return [(zc(0), None)]
        if s == half:
            return [(zc(half), ns - 2)]
        return [(zc(-s), 2 * s - 2), (zc(s), 2 * s - 1)]

    def z_first(l):
        for sub in range(3):
            for d in (RIGHT, LEFT):
                if active(l, sub, d, 1):
                    z_copy(l, sub, d, 1).start()

    def serve(l, s):
        for sub in range(3):
            for d in (RIGHT, LEFT):
                if not active(l, sub, d, s):
                    continue
                z_arrival(l, sub, d, s).wait_recv()
                if active(l, sub, d, s + 1):
                    if s >= 2:
                        z_copy(l, sub, d, s - 1).wait_send()
                    z_copy(l, sub, d, s + 1).start()
        if paired:
            for chunk, slot in hop_chunks(s):
                y_copy(l, chunk, slot, y_out_at).start()

    def z_drain(l):
        for sub in range(3):
            for d in (RIGHT, LEFT):
                last = half if active(l, sub, d, half) else half - 1
                for s in range(max(1, last - 1), last + 1):
                    z_copy(l, sub, d, s).wait_send()

    def y_wait(l, s):
        if paired and s > 0:
            for chunk, slot in hop_chunks(s):
                y_copy(l, chunk, slot, y_in_at).wait_recv()

    def y_drain(l):
        if paired:
            for s in range(1, half + 1):
                for chunk, slot in hop_chunks(s):
                    y_copy(l, chunk, slot, y_out_at).wait_send()

    def x_copy(l, chunk, slot, to):
        at = xg.at[l, chunk]
        return remote(at, at, x_send.at[l, slot], x_recv.at[l, chunk], tp=to)

    def x_begin(l):
        a, b = 2 * t, 2 * t + 1
        sends = ((a, 0, t_right), (b, 1, t_left), (b, 2, t_right), (a, 3, t_left), (a, 4, t_mate), (b, 5, t_mate))
        for chunk, slot, to in sends:
            x_copy(l, chunk, slot, to).start()
        return sends

    def x_middle(l):
        a, b, e, f = 2 * t_left, 2 * t_right + 1, 2 * t_left + 1, 2 * t_right
        sends = ((a, 6, t_right), (a, 7, t_mate), (b, 8, t_left), (b, 9, t_mate), (e, 10, t_mate), (f, 11, t_mate))
        arrived = []
        for chunk, slot, to in sends:
            if not any(chunk is other for other in arrived):
                x_copy(l, chunk, slot, to).wait_recv()
                arrived.append(chunk)
            x_copy(l, chunk, slot, to).start()
        return sends

    def x_far(l):
        a, b = 2 * t_opp, 2 * t_opp + 1
        sends = ((a, 12, t_mate), (b, 13, t_mate))
        for chunk, slot, to in sends:
            x_copy(l, chunk, slot, to).wait_recv()
            x_copy(l, chunk, slot, to).start()
        return sends

    def x_mate_wait(l, dx):
        for h in range(2):
            x_copy(l, 2 * chip(dx, 1 - c) + h, 0, t_mate).wait_recv()

    def stat_copies(buf, l, kind):
        copies = []
        for j in range(1, nt):
            to = lax.rem(t + j, nt)
            at = buf.at[l, t]
            copies.append(remote(at, at, s_send.at[l, kind, j - 1], s_recv.at[l, kind, j - 1], tp=to))
        return copies

    def stat_wait(buf, l, kind):
        for j in range(1, nt):
            at = buf.at[l, lax.rem(t + nt - j, nt)]
            remote(at, at, s_send.at[l, kind, j - 1], s_recv.at[l, kind, j - 1], tp=t_mate).wait_recv()

    def to_lanes(column):
        return jnp.broadcast_to(column, (tokens, 128)).T[:8]

    def to_column(row):
        return jnp.broadcast_to(row[:1], (128, tokens)).T

    def prepare(l):
        value = cur[...]
        squares = jnp.sum(value * value, axis=1, keepdims=True)
        rstat[l, t] = to_lanes(squares)
        scaled = (value * in_gain[l : l + 1, :]).astype(BF16)
        xg[l, 2 * t] = scaled[:, : scaled.shape[1] // 2]
        xg[l, 2 * t + 1] = scaled[:, scaled.shape[1] // 2 :]

    def accumulate(l, chunks, first):
        for sub, acc in ((0, acc_v), (1, acc_g)):
            total = None if first else acc[...]
            for chunk in chunks:
                part = mm(xg[l, chunk], wbuf[l, chunk, sub])
                total = part if total is None else total + part
            acc[...] = total

    block = 96

    def over_rows(body):
        def step(i, carry):
            body(pl.multiple_of(i * block, block))
            return carry

        lax.fori_loop(0, tokens // block, step, 0)

    def halo_copy(l):
        return remote(halo_out.at[l], halo_in.at[l], h_send.at[l], h_recv.at[l], sp=zc(1))

    reach = halo_out.shape[1]

    def gate(l):
        stat_wait(rstat, l, 0)
        total = rstat[l, 0]
        for j in range(1, nt):
            total = total + rstat[l, j]
        col_a[...] = to_column(lax.rsqrt(total / features + EPS))

        def body(at):
            rows = pl.ds(at, block)
            scale = both(col_a[rows, :])
            value = acc_v[rows, :] * scale
            gated = value * jax.nn.sigmoid(acc_g[rows, :] * scale)
            ext[pl.ds(pl.multiple_of(at + reach, 32), block), :] = gated.astype(BF16).astype(F32)

        over_rows(body)
        halo_out[l] = ext[tokens : tokens + reach, :].astype(BF16)
        halo_copy(l).start()

    def convolve(l):
        halo_copy(l).wait_recv()
        before = halo_in[l].astype(F32)
        ext[:reach, :] = jnp.where(z > 0, before, jnp.zeros_like(before))
        span = shifted.shape[1]
        for b in range(1, 8):
            shifted[b - 1] = ext[b : b + span, :]
        offset = reach - (n_taps - 1)

        def body(at):
            total = jnp.zeros((block // 4, ch), F32)
            return total

        small = 32

        def step(i, carry):
            at = pl.multiple_of(i * small, small)
            total = jnp.zeros((small, ch), F32)
            for k in range(n_taps):
                o = k + offset
                a, b = (o // 8) * 8, o % 8
                rows = pl.ds(pl.multiple_of(at + a, 8), small)
                window = ext[rows, :] if b == 0 else shifted[b - 1, rows, :]
                total = total + taps[l, k : k + 1, :] * window
            conved[pl.ds(at, small), :] = total
            return carry

        lax.fori_loop(0, tokens // small, step, 0)
        value = conved[...]
        sums = jnp.sum(value, axis=1, keepdims=True)
        spread = value - sums / ch
        cstat[l, t, :8] = to_lanes(sums)
        cstat[l, t, 8:] = to_lanes(jnp.sum(spread * spread, axis=1, keepdims=True))
        for copy in stat_copies(cstat, l, 1):
            copy.start()

    def normalize(l):
        stat_wait(cstat, l, 1)
        total = cstat[l, 0, :8]
        for j in range(1, nt):
            total = total + cstat[l, j, :8]
        mean = total / channels
        spread = jnp.zeros_like(mean)
        for j in range(nt):
            away = cstat[l, j, :8] / ch - mean
            spread = spread + (cstat[l, j, 8:] + ch * (away * away))
        col_a[...] = to_column(mean)
        col_b[...] = to_column(lax.rsqrt(spread / channels + EPS))

        def body(at):
            rows = pl.ds(at, block)
            normed = (conved[rows, :] - both(col_a[rows, :])) * both(col_b[rows, :])
            normed = normed * norm_gain[l : l + 1, :] + norm_shift[l : l + 1, :]
            mixed[rows, :] = (normed / (1.0 + jnp.exp(-normed))).astype(BF16)

        over_rows(body)

    def project(l, dx, core, h):
        return mm(mixed[...], wbuf[l, 2 * chip(dx, core) + h, 2])

    def p_copy(l, q):
        return remote(p_out.at[l, q], p_in.at[l, q], p_send.at[l, q], p_recv.at[l, q], tp=t_mate)

    def c_copy(l, slot):
        to = t_right if slot in (0, 2, 3) else t_left
        return remote(c_out.at[l, slot], c_in.at[l, slot], c_send.at[l, slot], c_recv.at[l, slot], tp=to)

    def give(l, dx, h):
        q = 2 * dx + h
        p_out[l, q] = project(l, dx, 1 - c, h).astype(BF16)
        p_copy(l, q).start()

    def pass_on(l, dx, h, slot, extra=None):
        q = 2 * dx + h
        total = project(l, dx, c, h)
        p_copy(l, q).wait_recv()
        total = total + p_in[l, q].astype(F32)
        if extra is not None:
            c_copy(l, extra).wait_recv()
            total = total + c_in[l, extra].astype(F32)
        c_out[l, slot] = total.astype(BF16)
        c_copy(l, slot).start()

    def settle(l, h, last):
        total = project(l, 0, c, h)
        p_copy(l, h).wait_recv()
        total = total + p_in[l, h].astype(F32)
        for slot in (2 + h, 4 + h):
            c_copy(l, slot).wait_recv()
            total = total + c_in[l, slot].astype(F32)
        cols = slice(h * ch, (h + 1) * ch)
        new = (cur[:, cols] + total).astype(BF16)
        if last:
            out[:, cols] = new
        else:
            cur[:, cols] = new.astype(F32)

    barrier = pltpu.get_barrier_semaphore()
    greeted = [{"tp": lax.rem(t + j, nt)} for j in range(1, nt)]
    greeted += [{"sp": zc(1)}, {"sp": zc(-1)}]
    if paired:
        greeted += [{"grp": y_mate}]
    for where in greeted:
        pl.semaphore_signal(barrier, inc=1, device_id=where, device_id_type=MESH)

    def local(l, sub):
        src = (w_value, w_gate, w_out)[sub]
        return pltpu.make_async_copy(src.at[l], wbuf.at[l, z, sub], local_sem.at[l, sub])

    for l in range(layers):
        for sub in range(3):
            local(l, sub).start()
    for sub in range(3):
        local(0, sub).wait()
    pl.semaphore_wait(barrier, len(greeted))

    z_first(0)
    cur[...] = hidden[...].astype(F32)
    prepare(0)
    x_sends = [[] for _ in range(layers)]
    x_sends[0] += x_begin(0)
    for copy in stat_copies(rstat, 0, 0):
        copy.start()
    serve(0, 1)
    x_sends[0] += x_middle(0)
    serve(0, 2)
    x_sends[0] += x_far(0)
    for dx in range(nx):
        x_mate_wait(0, dx)

    def ring_mm(l, s):
        y_wait(l, s)
        accumulate(l, [chunk for chunk, _ in hop_chunks(s)], s == 0)

    ring_mm(0, 0)
    ring_mm(0, 1)
    for s in range(3, half + 1):
        serve(0, s)
        if s == half - 1 and layers > 1:
            for sub in range(3):
                local(1, sub).wait()
            z_first(1)
        ring_mm(0, s - 1)
    ring_mm(0, half)

    for l in range(layers):
        last = l == layers - 1

        def more(s):
            if not last:
                serve(l + 1, s)

        gate(l)
        more(1)
        convolve(l)
        more(2)
        normalize(l)
        if last:
            for s in range(1, half + 1):
                pass
        give(l, 2, 0)
        give(l, 2, 1)
        give(l, 1, 1)
        pass_on(l, 2, 0, 0)
        pass_on(l, 2, 1, 1)
        give(l, 3, 0)
        pass_on(l, 1, 1, 3)
        give(l, 1, 0)
        pass_on(l, 3, 0, 4)
        more(3)
        give(l, 3, 1)
        give(l, 0, 0)
        give(l, 0, 1)
        pass_on(l, 1, 0, 2, 0)
        pass_on(l, 3, 1, 5, 1)
        more(4)
        settle(l, 0, last)
        settle(l, 1, last)
        if not last:
            n = l + 1
            prepare(n)
            x_sends[n] += x_begin(n)
            for copy in stat_copies(rstat, n, 0):
                copy.start()
            more(5)
            accumulate_done = False
            x_sends[n] += x_middle(n)
            more(6)
            x_sends[n] += x_far(n)
            more(7)
            more(8)
            for s in range(1, half + 1):
                y_wait(n, s)
            first = True
            for dx in (0, 1, -1, 2):
                accumulate(n, [2 * chip(dx, c), 2 * chip(dx, c) + 1], first)
                first = False
            for dx in (0, 1, -1, 2):
                x_mate_wait(n, dx)
                accumulate(n, [2 * chip(dx, 1 - c), 2 * chip(dx, 1 - c) + 1], False)

    for l in range(layers):
        z_drain(l)
        y_drain(l)
        for chunk, slot, to in x_sends[l]:
            x_copy(l, chunk, slot, to).wait_send()
        for copy in stat_copies(rstat, l, 0) + stat_copies(cstat, l, 1):
            copy.wait_send()
        halo_copy(l).wait_send()
        for q in range(2 * nx):
            p_copy(l, q).wait_send()
        for slot in range(6):
            c_copy(l, slot).wait_send()


def solution(mesh):
    sizes = (mesh.shape["grp"], mesh.shape["sp"], mesh.shape["tp"])
    groups, ns, nt = sizes

    def shards(hidden_in, in_gain, w_value, w_gate, conv_taps, norm_gain, norm_shift, w_out):
        layers, rows_w, ch = w_value.shape
        tokens = hidden_in.shape[0]
        vmem = pltpu.VMEM
        dma = pltpu.SemaphoreType.DMA
        half = ns // 2
        scratch = [
            vmem((layers, ns, 3, rows_w, ch), BF16),
            vmem((layers, 2 * nt, tokens, ch), BF16),
            vmem((tokens, 2 * ch), F32),
            vmem((tokens, ch), F32),
            vmem((tokens, ch), F32),
            vmem((tokens, 128), F32),
            vmem((tokens, 128), F32),
            vmem((layers, nt, 8, tokens), F32),
            vmem((layers, nt, 16, tokens), F32),
            vmem((layers, 32, ch), BF16),
            vmem((layers, 32, ch), BF16),
            vmem((tokens + 32, ch), F32),
            vmem((7, tokens + 24, ch), F32),
            vmem((tokens, ch), F32),
            vmem((tokens, ch), BF16),
            vmem((layers, nt, tokens, ch), BF16),
            vmem((layers, nt, tokens, ch), BF16),
            vmem((layers, 6, tokens, ch), BF16),
            vmem((layers, 6, tokens, ch), BF16),
            dma((layers, 3)),
            dma((layers, 3, 2, 2)),
            dma((layers, 3, 2, half)),
            dma((layers, ns - 1)),
            dma((layers, ns - 1)),
            dma((layers, 14)),
            dma((layers, 2 * nt)),
            dma((layers, 2, nt - 1)),
            dma((layers, 2, nt - 1)),
            dma((layers,)),
            dma((layers,)),
            dma((layers, nt)),
            dma((layers, nt)),
            dma((layers, 6)),
            dma((layers, 6)),
        ]
        v, a = pl.BlockSpec(memory_space=pltpu.VMEM), pl.BlockSpec(memory_space=pl.ANY)
        return pl.pallas_call(
            functools.partial(kernel, sizes),
            out_shape=jax.ShapeDtypeStruct(hidden_in.shape, hidden_in.dtype),
            in_specs=[v, v, a, a, v, v, v, a],
            out_specs=v,
            scratch_shapes=scratch,
            name="layers",
            compiler_params=pltpu.CompilerParams(
                collective_id=0, has_side_effects=True, vmem_limit_bytes=60 * 2**20
            ),
        )(hidden_in, in_gain, w_value, w_gate, conv_taps, norm_gain, norm_shift, w_out)

    placed = (
        P(("grp", "sp"), "tp"),
        P(None, "tp"),
        P(None, "sp", "tp"),
        P(None, "sp", "tp"),
        P(None, None, "tp"),
        P(None, "tp"),
        P(None, "tp"),
        P(None, "tp", "sp"),
    )
    return jax.shard_map(
        shards, mesh=mesh, in_specs=placed, out_specs=P(("grp", "sp"), "tp"), check_vma=False
    )
```

```python
import functools

import jax
import jax.numpy as jnp
from jax import lax
from jax.experimental import pallas as pl
from jax.experimental.pallas import tpu as pltpu
from jax.sharding import PartitionSpec as P

MESH = pl.DeviceIdType.MESH
EPS = 1e-06
F32 = jnp.float32
BF16 = jnp.bfloat16
RIGHT, LEFT = 1, -1


def mm(a, b):
    return jnp.dot(a, b, preferred_element_type=F32)


def both(col):
    return jnp.concatenate([col, col], axis=1)


def kernel(
    sizes,
    hidden,
    in_gain,
    w_value,
    w_gate,
    taps,
    norm_gain,
    norm_shift,
    w_out,
    out,
    start,
    wbuf,
    xg,
    cur,
    acc_v,
    acc_g,
    col_a,
    col_b,
    rstat,
    cstat,
    halo_out,
    halo_in,
    ext,
    shifted,
    conved,
    mixed,
    p_out,
    p_in,
    c_out,
    c_in,
    local_sem,
    z_send,
    z_recv,
    y_send,
    y_recv,
    x_send,
    x_recv,
    s_send,
    s_recv,
    h_send,
    h_recv,
    p_send,
    p_recv,
    c_send,
    c_recv,
):
    groups, ns, nt = sizes
    layers = w_value.shape[0]
    rows_w, ch = w_value.shape[1], w_value.shape[2]
    tokens = hidden.shape[0]
    n_taps = taps.shape[0]
    nx = nt // 2
    half = ns // 2
    channels = ch * nt
    features = hidden.shape[1] * nt
    z = lax.axis_index("sp")
    t = lax.axis_index("tp")
    paired = groups % 2 == 0
    x, c = t // 2, lax.rem(t, 2)

    def chip(dx, core):
        return 2 * lax.rem(x + dx + nx, nx) + core

    t_right, t_left, t_opp, t_mate = chip(1, c), chip(-1, c), chip(2, c), 2 * x + (1 - c)

    if paired:
        y = lax.axis_index("grp")
        par = lax.rem(y, 2)
        y_mate = y + 1 - 2 * par
        lone = 80
        ring_rows = rows_w - lone
        ring_base = par * lone
        y_out_at = pl.ds(pl.multiple_of(par * ring_rows, 16), lone)
        y_in_at = pl.ds(pl.multiple_of((1 - par) * ring_rows, 16), lone)
    else:
        ring_rows, ring_base = rows_w, 0

    def zc(offset):
        return lax.rem(z + offset + 2 * ns, ns)

    def remote(src, dst, ssem, rsem, **where):
        return pltpu.make_async_remote_copy(
            src_ref=src, dst_ref=dst, send_sem=ssem, recv_sem=rsem, device_id=where, device_id_type=MESH
        )

    cut = 96
    pieces = ((0, 0, ring_rows), (1, 0, ring_rows), (2, 0, cut), (2, cut, ring_rows - cut))
    early, late = (0, 1), (2, 3)

    def ring_part(l, chunk, p):
        sub, at, rows = pieces[p]
        return wbuf.at[l, chunk, sub, pl.ds(pl.multiple_of(ring_base + at, 16), rows), :]

    def z_copy(l, p, d, s):
        at, way = ring_part(l, zc(-d * (s - 1)), p), 0 if d == RIGHT else 1
        return remote(at, at, z_send.at[l], z_recv.at[l, p, way, s - 1], sp=zc(d))

    def z_arrival(l, p, d, s):
        at, way = ring_part(l, zc(-d * s), p), 0 if d == RIGHT else 1
        return remote(at, at, z_send.at[l], z_recv.at[l, p, way, s - 1], sp=zc(d))

    def active(l, p, d, s):
        if s < half:
            return True
        return s == half and d == (RIGHT, LEFT, RIGHT, LEFT)[p]

    bulk = half - 2

    def y_place(kind, d, s):
        if kind == 1:
            return 4
        if s <= bulk:
            return 0
        return 3 if s == half else (1 if d == RIGHT else 2)

    def y_copy(l, kind, d, s, rows):
        chunk = zc(-d * s)
        at = wbuf.at[l, chunk, pl.ds(0, 2), rows, :] if kind == 0 else wbuf.at[l, chunk, 2, rows, :]
        return remote(at, at, y_send.at[l], y_recv.at[l, y_place(kind, d, s)], grp=y_mate)

    def hop_ways(s):
        return (RIGHT, LEFT) if 0 < s < half else (RIGHT,)

    def z_first(l, which):
        for p in which:
            for d in (RIGHT, LEFT):
                if active(l, p, d, 1):
                    z_copy(l, p, d, 1).start()

    def serve(l, kind, s):
        for p in (early, late)[kind]:
            for d in (RIGHT, LEFT):
                if not active(l, p, d, s):
                    continue
                z_arrival(l, p, d, s).wait_recv()
                if active(l, p, d, s + 1):
                    z_copy(l, p, d, s + 1).start()
        if paired:
            for d in hop_ways(s):
                y_copy(l, kind, d, s, y_out_at).start()

    def z_drain(l):
        part = wbuf.at[l, pl.ds(0, ns - 1), :, pl.ds(0, ring_rows), :]
        pltpu.make_async_copy(part, part, z_send.at[l]).wait()

    def y_wait(l, kind, s):
        if not paired or s == 0:
            return
        if kind == 1:
            part = wbuf.at[l, pl.ds(0, ns - 1), 2, pl.ds(0, lone), :]
            pltpu.make_async_copy(part, part, y_recv.at[l, 4]).wait()
        elif s == bulk:
            part = wbuf.at[l, pl.ds(0, 2 * bulk), pl.ds(0, 2), pl.ds(0, lone), :]
            pltpu.make_async_copy(part, part, y_recv.at[l, 0]).wait()
        elif s > bulk:
            for d in hop_ways(s):
                y_copy(l, 0, d, s, y_in_at).wait_recv()

    def y_drain(l):
        if paired:
            part = wbuf.at[l, pl.ds(0, ns - 1), :, pl.ds(0, lone), :]
            pltpu.make_async_copy(part, part, y_send.at[l]).wait()

    def hop_chunks(s):
        if s == 0 or s == half:
            return [zc(s)]
        return [zc(-s), zc(s)]

    from_left, from_right, from_far, from_mate = 0, 2, 4, 6

    def x_copy(l, chunk, place, to):
        at = xg.at[l, chunk]
        return remote(at, at, x_send.at[l], x_recv.at[l, place], tp=to)

    def x_begin(l):
        a, b = 2 * t, 2 * t + 1
        x_copy(l, a, from_left, t_right).start()
        x_copy(l, b, from_right + 1, t_left).start()
        x_copy(l, b, from_left + 1, t_right).start()
        x_copy(l, a, from_right, t_left).start()
        x_copy(l, a, from_mate, t_mate).start()
        x_copy(l, b, from_mate, t_mate).start()

    def x_share(l, chunk, place):
        x_copy(l, chunk, place, t_mate).wait_recv()
        x_copy(l, chunk, from_mate, t_mate).start()

    def x_near(l):
        a, b = 2 * t_left, 2 * t_right + 1
        x_copy(l, a, from_left, t_mate).wait_recv()
        x_copy(l, a, from_far, t_right).start()
        x_copy(l, a, from_mate, t_mate).start()
        x_copy(l, b, from_right + 1, t_mate).wait_recv()
        x_copy(l, b, from_far + 1, t_left).start()
        x_copy(l, b, from_mate, t_mate).start()

    def x_rest(l):
        x_share(l, 2 * t_left + 1, from_left + 1)
        x_share(l, 2 * t_right, from_right)

    def x_far(l):
        x_share(l, 2 * t_opp, from_far)
        x_share(l, 2 * t_opp + 1, from_far + 1)

    def x_end(l):
        part = xg.at[l, pl.ds(0, nt)]
        pltpu.make_async_copy(part, part, x_recv.at[l, from_mate]).wait()

    def x_drain(l):
        part = xg.at[l, pl.ds(0, 14)]
        pltpu.make_async_copy(part, part, x_send.at[l]).wait()

    def stat_start(buf, l, kind):
        for j in range(1, nt):
            at = buf.at[l, t]
            remote(at, at, s_send.at[l, kind], s_recv.at[l, kind], tp=lax.rem(t + j, nt)).start()

    def stat_wait(buf, l, sem):
        part = buf.at[l, pl.ds(0, nt - 1)]
        pltpu.make_async_copy(part, part, sem).wait()

    groups_of = tokens // 128

    def to_lanes(column):
        wide = jnp.broadcast_to(column, (tokens, 128)).T[:8]
        row = lax.broadcasted_iota(jnp.int32, (8, 128), 0)
        tile = wide[:, :128]
        for i in range(1, groups_of):
            tile = jnp.where(row == i, wide[:, i * 128 : (i + 1) * 128], tile)
        return tile

    def to_column(tile):
        parts = [jnp.broadcast_to(tile[i : i + 1], (128, 128)).T for i in range(groups_of)]
        return jnp.concatenate(parts, axis=0)

    def prepare(l):
        value = cur[...]
        squares = jnp.sum(value * value, axis=1, keepdims=True)
        rstat[l, t] = to_lanes(squares)
        scaled = (value * in_gain[l : l + 1, :]).astype(BF16)
        xg[l, 2 * t] = scaled[:, : scaled.shape[1] // 2]
        xg[l, 2 * t + 1] = scaled[:, scaled.shape[1] // 2 :]

    def accumulate(l, chunks, first):
        for sub, acc in ((0, acc_v), (1, acc_g)):
            total = None if first else acc[...]
            for chunk in chunks:
                part = mm(xg[l, chunk], wbuf[l, chunk, sub])
                total = part if total is None else total + part
            acc[...] = total

    block = 96

    def over_rows(body):
        def step(i, carry):
            body(pl.multiple_of(i * block, block))
            return carry

        lax.fori_loop(0, tokens // block, step, 0)

    def halo_copy(l):
        return remote(halo_out.at[l], halo_in.at[l], h_send.at[l], h_recv.at[l], sp=zc(1))

    reach = halo_out.shape[1]

    def gate(l):
        stat_wait(rstat, l, s_recv.at[l, 0])
        total = rstat[l, 0]
        for j in range(1, nt):
            total = total + rstat[l, j]
        col_a[...] = to_column(lax.rsqrt(total / features + EPS))

        def body(at):
            rows = pl.ds(at, block)
            scale = both(col_a[rows, :])
            value = acc_v[rows, :] * scale
            gated = value * jax.nn.sigmoid(acc_g[rows, :] * scale)
            ext[pl.ds(pl.multiple_of(at + reach, 32), block), :] = gated.astype(BF16).astype(F32)

        over_rows(body)
        halo_out[l] = ext[tokens : tokens + reach, :].astype(BF16)
        halo_copy(l).start()

    small = 32

    def conv_rows(l, lo, hi):
        offset = reach - (n_taps - 1)

        def step(i, carry):
            at = pl.multiple_of(i * small, small)
            total = jnp.zeros((small, ch), F32)
            for k in range(n_taps):
                a, b = ((k + offset) // 8) * 8, (k + offset) % 8
                rows = pl.ds(pl.multiple_of(at + a, 8), small)
                window = ext[rows, :] if b == 0 else shifted[b - 1, rows, :]
                total = total + taps[k, l : l + 1, :] * window
            conved[pl.ds(at, small), :] = total
            return carry

        lax.fori_loop(lo, hi, step, 0)

    def conv_body(l):
        span = shifted.shape[1]
        for b in range(1, 8):
            shifted[b - 1, reach:, :] = ext[reach + b : span + b, :]
        conv_rows(l, 1, tokens // small)

    def conv_head(l):
        halo_copy(l).wait_recv()
        before = halo_in[l].astype(F32)
        ext[:reach, :] = jnp.where(z > 0, before, jnp.zeros_like(before))
        for b in range(1, 8):
            shifted[b - 1, :reach, :] = ext[b : reach + b, :]
        conv_rows(l, 0, 1)
        value = conved[...]
        sums = jnp.sum(value, axis=1, keepdims=True)
        spread = value - sums / ch
        cstat[l, t, 0] = to_lanes(sums)
        cstat[l, t, 1] = to_lanes(jnp.sum(spread * spread, axis=1, keepdims=True))
        stat_start(cstat, l, 1)

    def normalize(l):
        stat_wait(cstat, l, s_recv.at[l, 1])
        total = cstat[l, 0, 0]
        for j in range(1, nt):
            total = total + cstat[l, j, 0]
        mean = total / channels
        spread = jnp.zeros_like(mean)
        for j in range(nt):
            away = cstat[l, j, 0] / ch - mean
            spread = spread + (cstat[l, j, 1] + ch * (away * away))
        col_a[...] = to_column(mean)
        col_b[...] = to_column(lax.rsqrt(spread / channels + EPS))

        def body(at):
            rows = pl.ds(at, block)
            normed = (conved[rows, :] - both(col_a[rows, :])) * both(col_b[rows, :])
            normed = normed * norm_gain[l : l + 1, :] + norm_shift[l : l + 1, :]
            mixed[rows, :] = (normed / (1.0 + jnp.exp(-normed))).astype(BF16)

        over_rows(body)

    def project(l, dx, core, h):
        return mm(mixed[...], wbuf[l, 2 * chip(dx, core) + h, 2])

    def p_copy(l, q):
        return remote(p_out.at[l, q], p_in.at[l, q], p_send.at[l], p_recv.at[l, q], tp=t_mate)

    def c_copy(l, slot):
        to = t_right if slot in (0, 2, 3) else t_left
        return remote(c_out.at[l, slot], c_in.at[l, slot], c_send.at[l], c_recv.at[l, slot], tp=to)

    def give(l, dx, h):
        q = 2 * dx + h
        p_out[l, q] = project(l, dx, 1 - c, h).astype(BF16)
        p_copy(l, q).start()

    def pass_on(l, dx, h, slot, extra=None):
        q = 2 * dx + h
        total = project(l, dx, c, h)
        p_copy(l, q).wait_recv()
        total = total + p_in[l, q].astype(F32)
        if extra is not None:
            c_copy(l, extra).wait_recv()
            total = total + c_in[l, extra].astype(F32)
        c_out[l, slot] = total.astype(BF16)
        c_copy(l, slot).start()

    def settle(l, h, last):
        total = project(l, 0, c, h)
        p_copy(l, h).wait_recv()
        total = total + p_in[l, h].astype(F32)
        for slot in (2 + h, 4 + h):
            c_copy(l, slot).wait_recv()
            total = total + c_in[l, slot].astype(F32)
        cols = slice(h * ch, (h + 1) * ch)
        new = (cur[:, cols] + total).astype(BF16)
        if last:
            out[:, cols] = new
        else:
            cur[:, cols] = new.astype(F32)

    barrier = pltpu.get_barrier_semaphore()
    greeted = [{"tp": lax.rem(t + j, nt)} for j in range(1, nt)]
    greeted += [{"sp": zc(1)}, {"sp": zc(-1)}]
    if paired:
        greeted += [{"grp": y_mate}]
    for where in greeted:
        pl.semaphore_signal(barrier, inc=1, device_id=where, device_id_type=MESH)

    sources = (w_value, w_gate, w_out)
    load = pltpu.make_async_copy(hidden, start, local_sem.at[layers])
    load.start()
    for l in range(layers):
        for sub in range(3):
            pltpu.make_async_copy(sources[sub].at[l], wbuf.at[l, z, sub], local_sem.at[l]).start()

    def loaded(l):
        part = wbuf.at[l, z]
        pltpu.make_async_copy(part, part, local_sem.at[l]).wait()

    def ring_mm(l, s):
        y_wait(l, 0, s)
        if s == bulk:
            for back in range(1, bulk + 1):
                accumulate(l, hop_chunks(back), False)
        elif s == 0 or s > bulk:
            accumulate(l, hop_chunks(s), s == 0)

    loaded(0)
    pl.semaphore_wait(barrier, len(greeted))
    z_first(0, early)
    load.wait()
    cur[...] = start[...].astype(F32)
    prepare(0)
    x_begin(0)
    stat_start(rstat, 0, 0)
    lags = [3 if l == 0 else 4 for l in range(layers)]

    def step(l, s):
        if s <= half:
            serve(l, 0, s)
        if s > lags[l]:
            serve(l, 1, s - lags[l])
        if s == lags[l]:
            z_first(l, late)

    step(0, 1)
    step(0, 2)
    x_near(0)
    step(0, 3)
    x_rest(0)
    x_far(0)
    step(0, 4)
    x_end(0)
    ring_mm(0, 0)
    for s in range(5, half + 1):
        step(0, s)
        ring_mm(0, s - 1)
    ring_mm(0, half)

    for l in range(layers):
        final = l == layers - 1
        n = l + 1

        def more(s):
            if not final:
                step(n, s)

        gate(l)
        rest = list(range(half + 1, half + lags[l] + 1))
        step(l, rest[0])
        conv_body(l)
        step(l, rest[1])
        if not final:
            loaded(n)
            z_first(n, early)
        conv_head(l)
        for s in rest[2:]:
            step(l, s)
        normalize(l)
        more(1)
        y_wait(l, 1, half)
        give(l, 2, 0)
        give(l, 2, 1)
        give(l, 1, 1)
        pass_on(l, 2, 0, 0)
        pass_on(l, 2, 1, 1)
        give(l, 3, 0)
        pass_on(l, 1, 1, 3)
        give(l, 1, 0)
        pass_on(l, 3, 0, 4)
        give(l, 3, 1)
        more(2)
        give(l, 0, 0)
        give(l, 0, 1)
        more(3)
        pass_on(l, 1, 0, 2, 0)
        pass_on(l, 3, 1, 5, 1)
        more(4)
        settle(l, 0, final)
        settle(l, 1, final)
        if not final:
            prepare(n)
            x_begin(n)
            stat_start(rstat, n, 0)
            step(n, 5)
            x_near(n)
            step(n, 6)
            x_rest(n)
            x_far(n)
            step(n, 7)
            x_end(n)
            for s in range(7):
                ring_mm(n, s)
            step(n, half)
            ring_mm(n, half - 1)
            ring_mm(n, half)

    for l in range(layers):
        z_drain(l)
        y_drain(l)
        x_drain(l)
        stat_wait(rstat, l, s_send.at[l, 0])
        stat_wait(cstat, l, s_send.at[l, 1])
        halo_copy(l).wait_send()
        part = p_out.at[l]
        pltpu.make_async_copy(part, part, p_send.at[l]).wait()
        part = c_out.at[l]
        pltpu.make_async_copy(part, part, c_send.at[l]).wait()


def solution(mesh):
    sizes = (mesh.shape["grp"], mesh.shape["sp"], mesh.shape["tp"])
    groups, ns, nt = sizes

    def shards(hidden_in, in_gain, w_value, w_gate, conv_taps, norm_gain, norm_shift, w_out):
        layers, rows_w, ch = w_value.shape
        tokens = hidden_in.shape[0]
        vmem = pltpu.VMEM
        dma = pltpu.SemaphoreType.DMA
        half = ns // 2
        scratch = [
            vmem(hidden_in.shape, BF16),
            vmem((layers, ns, 3, rows_w, ch), BF16),
            vmem((layers, 2 * nt, tokens, ch), BF16),
            vmem((tokens, 2 * ch), F32),
            vmem((tokens, ch), F32),
            vmem((tokens, ch), F32),
            vmem((tokens, 128), F32),
            vmem((tokens, 128), F32),
            vmem((layers, nt, 8, 128), F32),
            vmem((layers, nt, 2, 8, 128), F32),
            vmem((layers, 32, ch), BF16),
            vmem((layers, 32, ch), BF16),
            vmem((tokens + 32, ch), F32),
            vmem((7, tokens + 24, ch), F32),
            vmem((tokens, ch), F32),
            vmem((tokens, ch), BF16),
            vmem((layers, nt, tokens, ch), BF16),
            vmem((layers, nt, tokens, ch), BF16),
            vmem((layers, 6, tokens, ch), BF16),
            vmem((layers, 6, tokens, ch), BF16),
            dma((layers + 1,)),
            dma((layers,)),
            dma((layers, 4, 2, half)),
            dma((layers,)),
            dma((layers, 5)),
            dma((layers,)),
            dma((layers, 7)),
            dma((layers, 2)),
            dma((layers, 2)),
            dma((layers,)),
            dma((layers,)),
            dma((layers,)),
            dma((layers, nt)),
            dma((layers,)),
            dma((layers, 6)),
        ]
        v, a = pl.BlockSpec(memory_space=pltpu.VMEM), pl.BlockSpec(memory_space=pl.ANY)
        return pl.pallas_call(
            functools.partial(kernel, sizes),
            out_shape=jax.ShapeDtypeStruct(hidden_in.shape, hidden_in.dtype),
            in_specs=[a, v, a, a, v, v, v, a],
            out_specs=v,
            scratch_shapes=scratch,
            name="layers",
            compiler_params=pltpu.CompilerParams(
                collective_id=0, has_side_effects=True, vmem_limit_bytes=60 * 2**20
            ),
        )(hidden_in, in_gain, w_value, w_gate, jnp.transpose(conv_taps, (1, 0, 2)), norm_gain, norm_shift, w_out)

    placed = (
        P(("grp", "sp"), "tp"),
        P(None, "tp"),
        P(None, "sp", "tp"),
        P(None, "sp", "tp"),
        P(None, None, "tp"),
        P(None, "tp"),
        P(None, "tp"),
        P(None, "tp", "sp"),
    )
    return jax.shard_map(
        shards, mesh=mesh, in_specs=placed, out_specs=P(("grp", "sp"), "tp"), check_vma=False
    )
```

```python
import functools

import jax
import jax.numpy as jnp
from jax import lax
from jax.experimental import pallas as pl
from jax.experimental.pallas import tpu as pltpu
from jax.sharding import PartitionSpec as P

MESH = pl.DeviceIdType.MESH
EPS = 1e-06
F32 = jnp.float32
BF16 = jnp.bfloat16
RIGHT, LEFT = 1, -1


def mm(a, b):
    return jnp.dot(a, b, preferred_element_type=F32)


def both(col):
    return jnp.concatenate([col, col], axis=1)


def kernel(
    sizes,
    hidden,
    in_gain,
    w_value,
    w_gate,
    taps,
    norm_gain,
    norm_shift,
    w_out,
    out,
    start,
    wbuf,
    xg,
    cur,
    acc_v,
    acc_g,
    col_a,
    col_b,
    rstat,
    cstat,
    halo_out,
    halo_in,
    ext,
    shifted,
    conved,
    mixed,
    p_out,
    p_in,
    c_out,
    c_in,
    local_sem,
    z_send,
    z_recv,
    y_send,
    g_send,
    w_recv,
    m_send,
    m_recv,
    x_send,
    x_recv,
    s_send,
    s_recv,
    h_send,
    h_recv,
    p_send,
    p_recv,
    c_send,
    c_recv,
):
    groups, ns, nt = sizes
    layers = w_value.shape[0]
    rows_w, ch = w_value.shape[1], w_value.shape[2]
    tokens = hidden.shape[0]
    n_taps = taps.shape[0]
    nx = nt // 2
    half = ns // 2
    channels = ch * nt
    features = hidden.shape[1] * nt
    z = lax.axis_index("sp")
    t = lax.axis_index("tp")
    paired = groups % 2 == 0
    x, c = t // 2, lax.rem(t, 2)

    def chip(dx, core):
        return 2 * lax.rem(x + dx + nx, nx) + core

    t_right, t_left, t_opp, t_mate = chip(1, c), chip(-1, c), chip(2, c), 2 * x + (1 - c)

    if paired:
        y = lax.axis_index("grp")
        par = lax.rem(y, 2)
        y_mate = y + 1 - 2 * par
        lone = 80
        ring_rows = rows_w - lone
        ring_base = par * lone
        y_out_at = pl.ds(pl.multiple_of(par * ring_rows, 16), lone)
        y_in_at = pl.ds(pl.multiple_of((1 - par) * ring_rows, 16), lone)
    else:
        ring_rows, ring_base = rows_w, 0

    def zc(offset):
        return lax.rem(z + offset + 2 * ns, ns)

    def remote(src, dst, ssem, rsem, **where):
        return pltpu.make_async_remote_copy(
            src_ref=src, dst_ref=dst, send_sem=ssem, recv_sem=rsem, device_id=where, device_id_type=MESH
        )

    early, late = (0, 1), (2,)
    first_core = c == 0
    second_core = c == 1

    def hand_over(l):
        return remote(wbuf.at[l, 0, z], wbuf.at[l, 1, z], m_send.at[l], m_recv.at[l], tp=t_mate)

    def ring_part(l, col, chunk, sub):
        return wbuf.at[l, col, chunk, sub, pl.ds(pl.multiple_of(ring_base, 16), ring_rows), :]

    def z_copy(l, col, sub, d, s):
        at, way = ring_part(l, col, zc(-d * (s - 1)), sub), 0 if d == RIGHT else 1
        return remote(at, at, z_send.at[l], z_recv.at[col, sub, way, s % 4], sp=zc(d))

    def z_arrival(l, col, sub, d, s):
        at, way = ring_part(l, col, zc(-d * s), sub), 0 if d == RIGHT else 1
        return remote(at, at, z_send.at[l], z_recv.at[col, sub, way, s % 4], sp=zc(d))

    def active(l, sub, d, s):
        if s < half:
            return True
        return s == half and d == (RIGHT, LEFT, RIGHT if l % 2 == 0 else LEFT)[sub]

    bulk = half - 2

    def place(kind, d, s):
        if kind == 1:
            return 4
        if s <= bulk:
            return 0
        return 3 if s == half else (1 if d == RIGHT else 2)

    def give_mate(l, kind, sub, d, s):
        chunk = zc(-d * s)
        src, dst = ring_part(l, 1, chunk, sub), ring_part(l, 0, chunk, sub)
        return remote(src, dst, g_send.at[l], w_recv.at[l, place(kind, d, s)], tp=t_mate)

    def y_copy(l, col, kind, d, s, rows):
        chunk = zc(-d * s)
        subs = pl.ds(0, 2) if kind == 0 else pl.ds(2, 1)
        src, dst = wbuf.at[l, col, chunk, subs, rows, :], wbuf.at[l, 0, chunk, subs, rows, :]
        where = {"grp": y_mate} if col == 0 else {"grp": y_mate, "tp": t_mate}
        return remote(src, dst, y_send.at[l], w_recv.at[l, place(kind, d, s)], **where)

    def hop_ways(s):
        return (RIGHT, LEFT) if 0 < s < half else (RIGHT,)

    def z_first(l, which):
        @pl.when(second_core)
        def _():
            for col in range(2):
                if col == 1 and which[0] == 0:
                    hand_over(l).wait_recv()
                for sub in which:
                    for d in (RIGHT, LEFT):
                        z_copy(l, col, sub, d, 1).start()

    def serve(l, kind, s):
        subs = (early, late)[kind]
        for sub in subs:
            for col in range(2):
                for d in (RIGHT, LEFT):
                    if not active(l, sub, d, s):
                        continue
                    z_arrival(l, col, sub, d, s).wait_recv()
                    if active(l, sub, d, s + 1):
                        z_copy(l, col, sub, d, s + 1).start()
                    if col == 1:
                        give_mate(l, kind, sub, d, s).start()
                    if paired and sub == subs[-1]:
                        y_copy(l, col, kind, d, s, y_out_at).start()

    def take(l, kind, s, rows):
        if s == 0:
            return
        if kind == 1:
            parts = [(wbuf.at[l, 0, pl.ds(0, ns - 1), 2, pl.ds(0, rows), :], 4)]
        elif s < bulk:
            return
        elif s == bulk:
            parts = [(wbuf.at[l, 0, pl.ds(0, 2 * bulk), pl.ds(0, 2), pl.ds(0, rows), :], 0)]
        else:
            parts = [(wbuf.at[l, 0, 0, pl.ds(0, 2), pl.ds(0, rows), :], place(0, d, s)) for d in hop_ways(s)]
        for part, sem in parts:
            pltpu.make_async_copy(part, part, w_recv.at[l, sem]).wait()

    def w_wait(l, kind, s):
        if paired:

            @pl.when(second_core)
            def _():
                take(l, kind, s, lone)

        @pl.when(first_core)
        def _():
            take(l, kind, s, rows_w)

    def w_drain(l):
        def wait(part, sem):
            pltpu.make_async_copy(part, part, sem).wait()

        @pl.when(second_core)
        def _():
            sent = wbuf.at[l, :, pl.ds(0, ns - 1), :, pl.ds(0, ring_rows), :]
            wait(sent, z_send.at[l])
            wait(sent.at[0], g_send.at[l])
            if paired:
                wait(wbuf.at[l, :, pl.ds(0, ns - 1), :, pl.ds(0, lone), :], y_send.at[l])

        @pl.when(first_core)
        def _():
            hand_over(l).wait_send()

    def hop_chunks(s):
        if s == 0 or s == half:
            return [zc(s)]
        return [zc(-s), zc(s)]

    from_left, from_right, from_far, from_mate = 0, 4, 8, 12

    def x_copy(l, chunk, where, to):
        at = xg.at[l, chunk]
        return remote(at, at, x_send.at[l], x_recv.at[where], tp=to)

    def x_two(l, owner):
        own = 2 * owner
        part = xg.at[l, pl.ds(own, 2)]
        return remote(part, part, x_send.at[l], x_recv.at[from_mate], tp=t_mate)

    def x_out(l, owner, k):
        a, b = 2 * owner, 2 * owner + 1
        x_copy(l, a, from_left + k, t_right).start()
        x_copy(l, b, from_right + k + 1, t_left).start()
        x_copy(l, b, from_left + k + 1, t_right).start()
        x_copy(l, a, from_right + k, t_left).start()

    def x_begin(l):
        x_two(l, t).start()

        @pl.when(first_core)
        def _():
            x_out(l, t, 0)
            x_two(l, t_mate).wait_recv()
            x_out(l, t_mate, 2)

    def x_share(l, chunk, where):
        x_copy(l, chunk, where, t_mate).wait_recv()
        x_copy(l, chunk, from_mate, t_mate).start()

    def x_gather(l):
        for k in (0, 2):
            core = k // 2
            a, b = 2 * chip(-1, core), 2 * chip(1, core) + 1
            x_copy(l, a, from_left + k, t_mate).wait_recv()
            x_copy(l, a, from_far + k, t_right).start()
            x_copy(l, a, from_mate, t_mate).start()
            x_copy(l, b, from_right + k + 1, t_mate).wait_recv()
            x_copy(l, b, from_far + k + 1, t_left).start()
            x_copy(l, b, from_mate, t_mate).start()
            x_share(l, 2 * chip(-1, core) + 1, from_left + k + 1)
            x_share(l, 2 * chip(1, core), from_right + k)
        for k in (0, 2):
            x_share(l, 2 * chip(2, k // 2), from_far + k)
            x_share(l, 2 * chip(2, k // 2) + 1, from_far + k + 1)

    def x_end(l):
        part = xg.at[l, pl.ds(0, 2 * nt - 2)]
        pltpu.make_async_copy(part, part, x_recv.at[from_mate]).wait()

    def x_drain(l):
        @pl.when(second_core)
        def _():
            x_two(l, t).wait_send()

        @pl.when(first_core)
        def _():
            for count in (2 * nt - 2, 12):
                part = xg.at[l, pl.ds(0, count)]
                pltpu.make_async_copy(part, part, x_send.at[l]).wait()

    def stat_start(buf, l, kind):
        for j in range(1, nt):
            at = buf.at[l, t]
            remote(at, at, s_send.at[l, kind], s_recv.at[kind], tp=lax.rem(t + j, nt)).start()

    def stat_wait(buf, l, sem):
        part = buf.at[l, pl.ds(0, nt - 1)]
        pltpu.make_async_copy(part, part, sem).wait()

    groups_of = tokens // 128

    def to_lanes(column):
        wide = jnp.broadcast_to(column, (tokens, 128)).T[:8]
        row = lax.broadcasted_iota(jnp.int32, (8, 128), 0)
        tile = wide[:, :128]
        for i in range(1, groups_of):
            tile = jnp.where(row == i, wide[:, i * 128 : (i + 1) * 128], tile)
        return tile

    def to_column(tile):
        parts = [jnp.broadcast_to(tile[i : i + 1], (128, 128)).T for i in range(groups_of)]
        return jnp.concatenate(parts, axis=0)

    def prepare(l):
        value = cur[...]
        squares = jnp.sum(value * value, axis=1, keepdims=True)
        rstat[l, t] = to_lanes(squares)
        scaled = (value * in_gain[l : l + 1, :]).astype(BF16)
        xg[l, 2 * t] = scaled[:, : scaled.shape[1] // 2]
        xg[l, 2 * t + 1] = scaled[:, scaled.shape[1] // 2 :]

    def accumulate(l, chunks, first):
        for sub, acc in ((0, acc_v), (1, acc_g)):
            total = None if first else acc[...]
            for chunk in chunks:
                part = mm(xg[l, chunk], wbuf[l, 0, chunk, sub])
                total = part if total is None else total + part
            acc[...] = total

    block = 96

    def over_rows(body):
        def step(i, carry):
            body(pl.multiple_of(i * block, block))
            return carry

        lax.fori_loop(0, tokens // block, step, 0)

    def halo_copy(l):
        return remote(halo_out.at[l], halo_in.at[l], h_send.at[l], h_recv.at[l], sp=zc(1))

    reach = halo_out.shape[1]

    def gate(l):
        stat_wait(rstat, l, s_recv.at[0])
        total = rstat[l, 0]
        for j in range(1, nt):
            total = total + rstat[l, j]
        col_a[...] = to_column(lax.rsqrt(total / features + EPS))

        def body(at):
            rows = pl.ds(at, block)
            scale = both(col_a[rows, :])
            value = acc_v[rows, :] * scale
            gated = value * jax.nn.sigmoid(acc_g[rows, :] * scale)
            ext[pl.ds(pl.multiple_of(at + reach, 32), block), :] = gated.astype(BF16).astype(F32)

        over_rows(body)
        halo_out[l] = ext[tokens : tokens + reach, :].astype(BF16)
        halo_copy(l).start()

    small = 32

    def conv_rows(l, lo, hi):
        offset = reach - (n_taps - 1)

        def step(i, carry):
            at = pl.multiple_of(i * small, small)
            total = jnp.zeros((small, ch), F32)
            for k in range(n_taps):
                a, b = ((k + offset) // 8) * 8, (k + offset) % 8
                rows = pl.ds(pl.multiple_of(at + a, 8), small)
                window = ext[rows, :] if b == 0 else shifted[b - 1, rows, :]
                total = total + taps[k, l : l + 1, :] * window
            conved[pl.ds(at, small), :] = total
            return carry

        lax.fori_loop(lo, hi, step, 0)

    def conv_body(l):
        span = shifted.shape[1]
        for b in range(1, 8):
            shifted[b - 1, reach:, :] = ext[reach + b : span + b, :]
        conv_rows(l, 1, tokens // small)

    def conv_head(l):
        halo_copy(l).wait_recv()
        before = halo_in[l].astype(F32)
        ext[:reach, :] = jnp.where(z > 0, before, jnp.zeros_like(before))
        for b in range(1, 8):
            shifted[b - 1, :reach, :] = ext[b : reach + b, :]
        conv_rows(l, 0, 1)
        value = conved[...]
        sums = jnp.sum(value, axis=1, keepdims=True)
        spread = value - sums / ch
        cstat[l, t, 0] = to_lanes(sums)
        cstat[l, t, 1] = to_lanes(jnp.sum(spread * spread, axis=1, keepdims=True))
        stat_start(cstat, l, 1)

    def normalize(l):
        stat_wait(cstat, l, s_recv.at[1])
        total = cstat[l, 0, 0]
        for j in range(1, nt):
            total = total + cstat[l, j, 0]
        mean = total / channels
        spread = jnp.zeros_like(mean)
        for j in range(nt):
            away = cstat[l, j, 0] / ch - mean
            spread = spread + (cstat[l, j, 1] + ch * (away * away))
        col_a[...] = to_column(mean)
        col_b[...] = to_column(lax.rsqrt(spread / channels + EPS))

        def body(at):
            rows = pl.ds(at, block)
            normed = (conved[rows, :] - both(col_a[rows, :])) * both(col_b[rows, :])
            normed = normed * norm_gain[l : l + 1, :] + norm_shift[l : l + 1, :]
            mixed[rows, :] = (normed / (1.0 + jnp.exp(-normed))).astype(BF16)

        over_rows(body)

    def project(l, dx, core, h):
        return mm(mixed[...], wbuf[l, 0, 2 * chip(dx, core) + h, 2])

    def p_copy(l, q):
        return remote(p_out.at[l, q], p_in.at[l, q], p_send.at[l], p_recv.at[q], tp=t_mate)

    def c_copy(l, slot):
        to = t_right if slot in (0, 2, 3) else t_left
        return remote(c_out.at[l, slot], c_in.at[l, slot], c_send.at[l], c_recv.at[slot], tp=to)

    def give(l, dx, h):
        q = 2 * dx + h
        p_out[l, q] = project(l, dx, 1 - c, h).astype(BF16)
        p_copy(l, q).start()

    def pass_on(l, dx, h, slot, extra=None):
        q = 2 * dx + h
        total = project(l, dx, c, h)
        p_copy(l, q).wait_recv()
        total = total + p_in[l, q].astype(F32)
        if extra is not None:
            c_copy(l, extra).wait_recv()
            total = total + c_in[l, extra].astype(F32)
        c_out[l, slot] = total.astype(BF16)
        c_copy(l, slot).start()

    def settle(l, h, last):
        total = project(l, 0, c, h)
        p_copy(l, h).wait_recv()
        total = total + p_in[l, h].astype(F32)
        for slot in (2 + h, 4 + h):
            c_copy(l, slot).wait_recv()
            total = total + c_in[l, slot].astype(F32)
        cols = slice(h * ch, (h + 1) * ch)
        new = (cur[:, cols] + total).astype(BF16)
        if last:
            out[:, cols] = new
        else:
            cur[:, cols] = new.astype(F32)

    barrier = pltpu.get_barrier_semaphore()
    greeted = [{"tp": lax.rem(t + j, nt)} for j in range(1, nt)]
    greeted += [{"sp": zc(1)}, {"sp": zc(-1)}]
    if paired:
        greeted += [{"grp": y_mate}, {"grp": y_mate, "tp": t_mate}]
    for where in greeted:
        pl.semaphore_signal(barrier, inc=1, device_id=where, device_id_type=MESH)

    sources = (w_value, w_gate, w_out)
    load = pltpu.make_async_copy(hidden, start, local_sem.at[layers])
    load.start()
    for l in range(layers):
        for sub in range(3):
            pltpu.make_async_copy(sources[sub].at[l], wbuf.at[l, 0, z, sub], local_sem.at[l]).start()

    def loaded(l):
        part = wbuf.at[l, 0, z]
        pltpu.make_async_copy(part, part, local_sem.at[l]).wait()

    def ring_mm(l, s):
        w_wait(l, 0, s)
        if s == bulk:
            for back in range(1, bulk + 1):
                accumulate(l, hop_chunks(back), False)
        elif s == 0 or s > bulk:
            accumulate(l, hop_chunks(s), s == 0)

    loaded(0)
    pl.semaphore_wait(barrier, len(greeted))

    @pl.when(first_core)
    def _():
        hand_over(0).start()

    z_first(0, early)
    load.wait()
    cur[...] = start[...].astype(F32)
    prepare(0)
    x_begin(0)
    stat_start(rstat, 0, 0)

    @pl.when(first_core)
    def _():
        for l in range(1, layers):
            loaded(l)
            hand_over(l).start()

    lags = [3 for l in range(layers)]

    def step(l, s):
        if s <= half:
            serve(l, 0, s)
        if s > lags[l]:
            serve(l, 1, s - lags[l])

    def steps(l, first, end):
        @pl.when(second_core)
        def _():
            for s in range(first, end):
                step(l, s)

        for s in range(first, end):
            if s == lags[l]:
                z_first(l, late)

    steps(0, 1, 4)
    steps(0, 4, 5)

    @pl.when(first_core)
    def _():
        x_gather(0)

    @pl.when(second_core)
    def _():
        x_end(0)

    ring_mm(0, 0)
    for s in range(5, half + 1):
        steps(0, s, s + 1)
        ring_mm(0, s - 1)
    steps(0, half + 1, half + 2)
    ring_mm(0, half)

    for l in range(layers):
        final = l == layers - 1
        n = l + 1

        def more(s):
            if not final:
                steps(n, s, s + 1)

        gate(l)
        rest = half + 2
        conv_body(l)
        steps(l, rest, rest + 1)
        if not final:

            @pl.when(second_core)
            def _():
                loaded(n)

            z_first(n, early)
        conv_head(l)
        steps(l, rest + 1, half + lags[l] + 1)
        normalize(l)
        more(1)
        w_wait(l, 1, half)
        give(l, 2, 0)
        give(l, 2, 1)
        give(l, 1, 1)
        pass_on(l, 2, 0, 0)
        pass_on(l, 2, 1, 1)
        give(l, 3, 0)
        pass_on(l, 1, 1, 3)
        give(l, 1, 0)
        pass_on(l, 3, 0, 4)
        give(l, 3, 1)
        give(l, 0, 0)
        give(l, 0, 1)
        more(2)
        pass_on(l, 1, 0, 2, 0)
        pass_on(l, 3, 1, 5, 1)
        more(3)
        more(4)
        settle(l, 0, final)
        settle(l, 1, final)
        if not final:
            prepare(n)
            x_begin(n)
            stat_start(rstat, n, 0)
            steps(n, 5, 8)

            @pl.when(first_core)
            def _():
                x_gather(n)

            @pl.when(second_core)
            def _():
                x_end(n)

            for s in range(7):
                ring_mm(n, s)
            steps(n, half, half + 1)
            ring_mm(n, half - 1)
            steps(n, half + 1, half + 2)
            ring_mm(n, half)

    for l in range(layers):
        w_drain(l)
        x_drain(l)
        stat_wait(rstat, l, s_send.at[l, 0])
        stat_wait(cstat, l, s_send.at[l, 1])
        halo_copy(l).wait_send()
        part = p_out.at[l]
        pltpu.make_async_copy(part, part, p_send.at[l]).wait()
        part = c_out.at[l]
        pltpu.make_async_copy(part, part, c_send.at[l]).wait()


def solution(mesh):
    sizes = (mesh.shape["grp"], mesh.shape["sp"], mesh.shape["tp"])
    groups, ns, nt = sizes

    def shards(hidden_in, in_gain, w_value, w_gate, conv_taps, norm_gain, norm_shift, w_out):
        layers, rows_w, ch = w_value.shape
        tokens = hidden_in.shape[0]
        vmem = pltpu.VMEM
        dma = pltpu.SemaphoreType.DMA
        half = ns // 2
        scratch = [
            vmem(hidden_in.shape, BF16),
            vmem((layers, 2, ns, 3, rows_w, ch), BF16),
            vmem((layers, 2 * nt, tokens, ch), BF16),
            vmem((tokens, 2 * ch), F32),
            vmem((tokens, ch), F32),
            vmem((tokens, ch), F32),
            vmem((tokens, 128), F32),
            vmem((tokens, 128), F32),
            vmem((layers, nt, 8, 128), F32),
            vmem((layers, nt, 2, 8, 128), F32),
            vmem((layers, 32, ch), BF16),
            vmem((layers, 32, ch), BF16),
            vmem((tokens + 32, ch), F32),
            vmem((7, tokens + 24, ch), F32),
            vmem((tokens, ch), F32),
            vmem((tokens, ch), BF16),
            vmem((layers, nt, tokens, ch), BF16),
            vmem((layers, nt, tokens, ch), BF16),
            vmem((layers, 6, tokens, ch), BF16),
            vmem((layers, 6, tokens, ch), BF16),
            dma((layers + 1,)),
            dma((layers,)),
            dma((2, 3, 2, 4)),
            dma((layers,)),
            dma((layers,)),
            dma((layers, 5)),
            dma((layers,)),
            dma((layers,)),
            dma((layers,)),
            dma((13,)),
            dma((layers, 2)),
            dma((2,)),
            dma((layers,)),
            dma((layers,)),
            dma((layers,)),
            dma((nt,)),
            dma((layers,)),
            dma((6,)),
        ]
        v, a = pl.BlockSpec(memory_space=pltpu.VMEM), pl.BlockSpec(memory_space=pl.ANY)
        return pl.pallas_call(
            functools.partial(kernel, sizes),
            out_shape=jax.ShapeDtypeStruct(hidden_in.shape, hidden_in.dtype),
            in_specs=[a, v, a, a, v, v, v, a],
            out_specs=v,
            scratch_shapes=scratch,
            name="layers",
            compiler_params=pltpu.CompilerParams(
                collective_id=0, has_side_effects=True, vmem_limit_bytes=60 * 2**20
            ),
        )(hidden_in, in_gain, w_value, w_gate, jnp.transpose(conv_taps, (1, 0, 2)), norm_gain, norm_shift, w_out)

    placed = (
        P(("grp", "sp"), "tp"),
        P(None, "tp"),
        P(None, "sp", "tp"),
        P(None, "sp", "tp"),
        P(None, None, "tp"),
        P(None, "tp"),
        P(None, "tp"),
        P(None, "tp", "sp"),
    )
    return jax.shard_map(
        shards, mesh=mesh, in_specs=placed, out_specs=P(("grp", "sp"), "tp"), check_vma=False
    )
```

```python
import functools

import jax
import jax.numpy as jnp
from jax import lax
from jax.experimental import pallas as pl
from jax.experimental.pallas import tpu as pltpu
from jax.sharding import PartitionSpec as P

MESH = pl.DeviceIdType.MESH
EPS = 1e-06
F32 = jnp.float32
BF16 = jnp.bfloat16
RIGHT, LEFT = 1, -1


def mm(a, b):
    return jnp.dot(a, b, preferred_element_type=F32)


def both(col):
    return jnp.concatenate([col, col], axis=1)


def kernel(
    sizes,
    hidden,
    in_gain_in,
    w_value,
    w_gate,
    taps_in,
    norm_gain_in,
    norm_shift_in,
    w_out,
    out,
    in_gain,
    taps,
    norm_gain,
    norm_shift,
    result,
    start,
    wbuf,
    xg,
    cur,
    acc_v,
    acc_g,
    col_a,
    col_b,
    rstat,
    cstat,
    halo_out,
    halo_in,
    ext,
    shifted,
    conved,
    mixed,
    p_out,
    p_in,
    c_out,
    c_in,
    local_sem,
    out_sem,
    z_send,
    z_recv,
    y_send,
    g_send,
    w_recv,
    m_send,
    m_recv,
    x_send,
    x_recv,
    s_send,
    s_recv,
    h_send,
    h_recv,
    p_send,
    p_recv,
    c_send,
    c_recv,
):
    groups, ns, nt = sizes
    layers = w_value.shape[0]
    rows_w, ch = w_value.shape[1], w_value.shape[2]
    tokens = hidden.shape[0]
    n_taps = taps.shape[0]
    nx = nt // 2
    half = ns // 2
    channels = ch * nt
    features = hidden.shape[1] * nt
    z = lax.axis_index("sp")
    t = lax.axis_index("tp")
    paired = groups % 2 == 0
    x, c = t // 2, lax.rem(t, 2)

    def chip(dx, core):
        return 2 * lax.rem(x + dx + nx, nx) + core

    t_right, t_left, t_opp, t_mate = chip(1, c), chip(-1, c), chip(2, c), 2 * x + (1 - c)

    if paired:
        y = lax.axis_index("grp")
        par = lax.rem(y, 2)
        y_mate = y + 1 - 2 * par
        lone = 80
        ring_rows = rows_w - lone
        ring_base = par * lone
        y_out_at = pl.ds(pl.multiple_of(par * ring_rows, 16), lone)
        y_in_at = pl.ds(pl.multiple_of((1 - par) * ring_rows, 16), lone)
    else:
        ring_rows, ring_base = rows_w, 0

    def zc(offset):
        return lax.rem(z + offset + 2 * ns, ns)

    def remote(src, dst, ssem, rsem, **where):
        return pltpu.make_async_remote_copy(
            src_ref=src, dst_ref=dst, send_sem=ssem, recv_sem=rsem, device_id=where, device_id_type=MESH
        )

    early, late = (0, 1), (2,)
    first_core = c == 0
    second_core = c == 1

    def hand_over(l):
        return remote(wbuf.at[l, 0, z], wbuf.at[l, 1, z], m_send.at[l], m_recv.at[l], tp=t_mate)

    def ring_part(l, col, chunk, sub):
        return wbuf.at[l, col, chunk, sub, pl.ds(pl.multiple_of(ring_base, 16), ring_rows), :]

    def z_copy(l, col, sub, d, s):
        at, way = ring_part(l, col, zc(-d * (s - 1)), sub), 0 if d == RIGHT else 1
        return remote(at, at, z_send.at[l], z_recv.at[col, sub, way, s % 4], sp=zc(d))

    def z_arrival(l, col, sub, d, s):
        at, way = ring_part(l, col, zc(-d * s), sub), 0 if d == RIGHT else 1
        return remote(at, at, z_send.at[l], z_recv.at[col, sub, way, s % 4], sp=zc(d))

    def active(l, sub, d, s):
        if s < half:
            return True
        return s == half and d == (RIGHT, LEFT, RIGHT if l % 2 == 0 else LEFT)[sub]

    bulk = half - 2

    def place(kind, d, s):
        if kind == 1:
            return 4
        if s <= bulk:
            return 0
        return 3 if s == half else (1 if d == RIGHT else 2)

    def give_mate(l, kind, sub, d, s):
        chunk = zc(-d * s)
        src, dst = ring_part(l, 1, chunk, sub), ring_part(l, 0, chunk, sub)
        return remote(src, dst, g_send.at[l], w_recv.at[l, place(kind, d, s)], tp=t_mate)

    def y_copy(l, col, kind, d, s, rows):
        chunk = zc(-d * s)
        subs = pl.ds(0, 2) if kind == 0 else pl.ds(2, 1)
        src, dst = wbuf.at[l, col, chunk, subs, rows, :], wbuf.at[l, 0, chunk, subs, rows, :]
        where = {"grp": y_mate} if col == 0 else {"grp": y_mate, "tp": t_mate}
        return remote(src, dst, y_send.at[l], w_recv.at[l, place(kind, d, s)], **where)

    def hop_ways(s):
        return (RIGHT, LEFT) if 0 < s < half else (RIGHT,)

    def z_first(l, which):
        @pl.when(second_core)
        def _():
            first = which[0] == 0
            if first and l > 0:
                hand_over(l).wait_recv()
            for col in (0, 1) if first and l == 0 else (1, 0):
                if first and l == 0 and col == 1:
                    hand_over(l).wait_recv()
                for sub in which:
                    for d in (RIGHT, LEFT):
                        z_copy(l, col, sub, d, 1).start()

    def serve(l, kind, s, some=None):
        subs = (early, late)[kind]
        for sub in some or subs:
            for col in (1, 0):
                for d in (RIGHT, LEFT):
                    if not active(l, sub, d, s):
                        continue
                    z_arrival(l, col, sub, d, s).wait_recv()
                    if active(l, sub, d, s + 1):
                        z_copy(l, col, sub, d, s + 1).start()
                    if col == 1:
                        give_mate(l, kind, sub, d, s).start()
                    if paired and sub == subs[-1]:
                        y_copy(l, col, kind, d, s, y_out_at).start()

    def take(l, kind, s, rows):
        if s == 0:
            return
        if kind == 1:
            parts = [(wbuf.at[l, 0, pl.ds(0, ns - 1), 2, pl.ds(0, rows), :], 4)]
        elif s < bulk:
            return
        elif s == bulk:
            parts = [(wbuf.at[l, 0, pl.ds(0, 2 * bulk), pl.ds(0, 2), pl.ds(0, rows), :], 0)]
        else:
            parts = [(wbuf.at[l, 0, 0, pl.ds(0, 2), pl.ds(0, rows), :], place(0, d, s)) for d in hop_ways(s)]
        for part, sem in parts:
            pltpu.make_async_copy(part, part, w_recv.at[l, sem]).wait()

    def w_wait(l, kind, s):
        if paired:

            @pl.when(second_core)
            def _():
                take(l, kind, s, lone)

        @pl.when(first_core)
        def _():
            take(l, kind, s, rows_w)

    def w_drain(l):
        def wait(part, sem):
            pltpu.make_async_copy(part, part, sem).wait()

        @pl.when(second_core)
        def _():
            sent = wbuf.at[l, :, pl.ds(0, ns - 1), :, pl.ds(0, ring_rows), :]
            wait(sent, z_send.at[l])
            wait(sent.at[0], g_send.at[l])
            if paired:
                wait(wbuf.at[l, :, pl.ds(0, ns - 1), :, pl.ds(0, lone), :], y_send.at[l])

        @pl.when(first_core)
        def _():
            hand_over(l).wait_send()

    def hop_chunks(s):
        if s == 0 or s == half:
            return [zc(s)]
        return [zc(-s), zc(s)]

    from_left, from_right, from_far, from_mate = 0, 4, 8, 12

    def x_copy(l, chunk, where, to):
        at = xg.at[l, chunk]
        return remote(at, at, x_send.at[l], x_recv.at[where], tp=to)

    def x_two(l, owner):
        own = 2 * owner
        part = xg.at[l, pl.ds(own, 2)]
        return remote(part, part, x_send.at[l], x_recv.at[from_mate], tp=t_mate)

    def x_out(l, owner, k):
        a, b = 2 * owner, 2 * owner + 1
        x_copy(l, a, from_left + k, t_right).start()
        x_copy(l, b, from_right + k + 1, t_left).start()
        x_copy(l, b, from_left + k + 1, t_right).start()
        x_copy(l, a, from_right + k, t_left).start()

    def x_begin(l):
        x_two(l, t).start()

        @pl.when(first_core)
        def _():
            x_out(l, t, 0)
            x_two(l, t_mate).wait_recv()
            x_out(l, t_mate, 2)

    def x_share(l, chunk, where):
        x_copy(l, chunk, where, t_mate).wait_recv()
        x_copy(l, chunk, from_mate, t_mate).start()

    def x_gather(l):
        for k in (0, 2):
            core = k // 2
            a, b = 2 * chip(-1, core), 2 * chip(1, core) + 1
            x_copy(l, a, from_left + k, t_mate).wait_recv()
            x_copy(l, a, from_far + k, t_right).start()
            x_copy(l, a, from_mate, t_mate).start()
            x_copy(l, b, from_right + k + 1, t_mate).wait_recv()
            x_copy(l, b, from_far + k + 1, t_left).start()
            x_copy(l, b, from_mate, t_mate).start()
            x_share(l, 2 * chip(-1, core) + 1, from_left + k + 1)
            x_share(l, 2 * chip(1, core), from_right + k)
        for k in (0, 2):
            x_share(l, 2 * chip(2, k // 2), from_far + k)
            x_share(l, 2 * chip(2, k // 2) + 1, from_far + k + 1)

    def x_end(l):
        part = xg.at[l, pl.ds(0, 2 * nt - 2)]
        pltpu.make_async_copy(part, part, x_recv.at[from_mate]).wait()

    def x_drain(l):
        @pl.when(second_core)
        def _():
            x_two(l, t).wait_send()

        @pl.when(first_core)
        def _():
            for count in (2 * nt - 2, 12):
                part = xg.at[l, pl.ds(0, count)]
                pltpu.make_async_copy(part, part, x_send.at[l]).wait()

    def stat_start(buf, l, kind):
        for j in range(1, nt):
            at = buf.at[l, t]
            remote(at, at, s_send.at[l, kind], s_recv.at[kind], tp=lax.rem(t + j, nt)).start()

    def stat_wait(buf, l, sem):
        part = buf.at[l, pl.ds(0, nt - 1)]
        pltpu.make_async_copy(part, part, sem).wait()

    groups_of = tokens // 128

    def to_lanes(column):
        wide = jnp.broadcast_to(column, (tokens, 128)).T[:8]
        row = lax.broadcasted_iota(jnp.int32, (8, 128), 0)
        tile = wide[:, :128]
        for i in range(1, groups_of):
            tile = jnp.where(row == i, wide[:, i * 128 : (i + 1) * 128], tile)
        return tile

    def to_column(tile):
        parts = [jnp.broadcast_to(tile[i : i + 1], (128, 128)).T for i in range(groups_of)]
        return jnp.concatenate(parts, axis=0)

    def prepare(l):
        value = cur[...]
        squares = jnp.sum(value * value, axis=1, keepdims=True)
        rstat[l, t] = to_lanes(squares)
        scaled = (value * in_gain[l : l + 1, :]).astype(BF16)
        xg[l, 2 * t] = scaled[:, : scaled.shape[1] // 2]
        xg[l, 2 * t + 1] = scaled[:, scaled.shape[1] // 2 :]

    def accumulate(l, chunks, first):
        for sub, acc in ((0, acc_v), (1, acc_g)):
            total = None if first else acc[...]
            for chunk in chunks:
                part = mm(xg[l, chunk], wbuf[l, 0, chunk, sub])
                total = part if total is None else total + part
            acc[...] = total

    block = 96

    def over_rows(body):
        def step(i, carry):
            body(pl.multiple_of(i * block, block))
            return carry

        lax.fori_loop(0, tokens // block, step, 0)

    def halo_copy(l):
        return remote(halo_out.at[l], halo_in.at[l], h_send.at[l], h_recv.at[l], sp=zc(1))

    reach = halo_out.shape[1]

    def gate(l):
        stat_wait(rstat, l, s_recv.at[0])
        total = rstat[l, 0]
        for j in range(1, nt):
            total = total + rstat[l, j]
        col_a[...] = to_column(lax.rsqrt(total / features + EPS))

        def body(at):
            rows = pl.ds(at, block)
            scale = both(col_a[rows, :])
            value = acc_v[rows, :] * scale
            gated = value * jax.nn.sigmoid(acc_g[rows, :] * scale)
            ext[pl.ds(pl.multiple_of(at + reach, 32), block), :] = gated.astype(BF16).astype(F32)

        over_rows(body)
        halo_out[l] = ext[tokens : tokens + reach, :].astype(BF16)
        halo_copy(l).start()

    small = 32

    def conv_rows(l, lo, hi):
        offset = reach - (n_taps - 1)

        def step(i, carry):
            at = pl.multiple_of(i * small, small)
            total = jnp.zeros((small, ch), F32)
            for k in range(n_taps):
                a, b = ((k + offset) // 8) * 8, (k + offset) % 8
                rows = pl.ds(pl.multiple_of(at + a, 8), small)
                window = ext[rows, :] if b == 0 else shifted[b - 1, rows, :]
                total = total + taps[k, l : l + 1, :] * window
            conved[pl.ds(at, small), :] = total
            return carry

        lax.fori_loop(lo, hi, step, 0)

    def conv_body(l):
        span = shifted.shape[1]
        for b in range(1, 8):
            shifted[b - 1, reach:, :] = ext[reach + b : span + b, :]
        conv_rows(l, 1, tokens // small)

    def conv_head(l):
        halo_copy(l).wait_recv()
        before = halo_in[l].astype(F32)
        ext[:reach, :] = jnp.where(z > 0, before, jnp.zeros_like(before))
        for b in range(1, 8):
            shifted[b - 1, :reach, :] = ext[b : reach + b, :]
        conv_rows(l, 0, 1)
        value = conved[...]
        sums = jnp.sum(value, axis=1, keepdims=True)
        spread = value - sums / ch
        cstat[l, t, 0] = to_lanes(sums)
        cstat[l, t, 1] = to_lanes(jnp.sum(spread * spread, axis=1, keepdims=True))
        stat_start(cstat, l, 1)

    def normalize(l):
        stat_wait(cstat, l, s_recv.at[1])
        total = cstat[l, 0, 0]
        for j in range(1, nt):
            total = total + cstat[l, j, 0]
        mean = total / channels
        spread = jnp.zeros_like(mean)
        for j in range(nt):
            away = cstat[l, j, 0] / ch - mean
            spread = spread + (cstat[l, j, 1] + ch * (away * away))
        col_a[...] = to_column(mean)
        col_b[...] = to_column(lax.rsqrt(spread / channels + EPS))

        def body(at):
            rows = pl.ds(at, block)
            normed = (conved[rows, :] - both(col_a[rows, :])) * both(col_b[rows, :])
            normed = normed * norm_gain[l : l + 1, :] + norm_shift[l : l + 1, :]
            mixed[rows, :] = (normed / (1.0 + jnp.exp(-normed))).astype(BF16)

        over_rows(body)

    def project(l, dx, core, h):
        return mm(mixed[...], wbuf[l, 0, 2 * chip(dx, core) + h, 2])

    def p_copy(l, q):
        return remote(p_out.at[l, q], p_in.at[l, q], p_send.at[l], p_recv.at[q], tp=t_mate)

    def c_copy(l, slot):
        to = t_right if slot in (0, 2, 3) else t_left
        return remote(c_out.at[l, slot], c_in.at[l, slot], c_send.at[l], c_recv.at[slot], tp=to)

    def give(l, dx, h):
        q = 2 * dx + h
        p_out[l, q] = project(l, dx, 1 - c, h).astype(BF16)
        p_copy(l, q).start()

    def pass_on(l, dx, h, slot, extra=None):
        q = 2 * dx + h
        total = project(l, dx, c, h)
        p_copy(l, q).wait_recv()
        total = total + p_in[l, q].astype(F32)
        if extra is not None:
            c_copy(l, extra).wait_recv()
            total = total + c_in[l, extra].astype(F32)
        c_out[l, slot] = total.astype(BF16)
        c_copy(l, slot).start()

    def settle(l, h, last):
        total = project(l, 0, c, h)
        p_copy(l, h).wait_recv()
        total = total + p_in[l, h].astype(F32)
        for slot in (2 + h, 4 + h):
            c_copy(l, slot).wait_recv()
            total = total + c_in[l, slot].astype(F32)
        cols = slice(h * ch, (h + 1) * ch)
        new = (cur[:, cols] + total).astype(BF16)
        if last:
            result[h] = new
            pltpu.make_async_copy(result.at[h], out.at[:, cols], out_sem.at[h]).start()
        else:
            cur[:, cols] = new.astype(F32)

    barrier = pltpu.get_barrier_semaphore()
    greeted = [{"tp": lax.rem(t + j, nt)} for j in range(1, nt)]
    greeted += [{"sp": zc(1)}, {"sp": zc(-1)}]
    if paired:
        greeted += [{"grp": y_mate}, {"grp": y_mate, "tp": t_mate}]
    for where in greeted:
        pl.semaphore_signal(barrier, inc=1, device_id=where, device_id_type=MESH)

    sources = (w_value, w_gate, w_out)
    loads = [
        pltpu.make_async_copy(src, dst, local_sem.at[layers + i])
        for i, (src, dst) in enumerate(
            (
                (hidden, start),
                (in_gain_in, in_gain),
                (taps_in, taps),
                (norm_gain_in, norm_gain),
                (norm_shift_in, norm_shift),
            )
        )
    ]
    for l in range(layers):
        for sub in range(3):
            pltpu.make_async_copy(sources[sub].at[l], wbuf.at[l, 0, z, sub], local_sem.at[l]).start()
        if l == 0:
            for load in loads:
                load.start()

    def loaded(l):
        part = wbuf.at[l, 0, z]
        pltpu.make_async_copy(part, part, local_sem.at[l]).wait()

    def ring_mm(l, s):
        w_wait(l, 0, s)
        if s == bulk:
            for back in range(1, bulk + 1):
                accumulate(l, hop_chunks(back), False)
        elif s == 0 or s > bulk:
            accumulate(l, hop_chunks(s), s == 0)

    loaded(0)
    pl.semaphore_wait(barrier, len(greeted))

    @pl.when(first_core)
    def _():
        hand_over(0).start()

    z_first(0, early)
    for load in loads:
        load.wait()
    cur[...] = start[...].astype(F32)
    prepare(0)
    x_begin(0)
    stat_start(rstat, 0, 0)

    @pl.when(first_core)
    def _():
        for l in range(1, layers):
            loaded(l)
            hand_over(l).start()

    lags = [3 for l in range(layers)]

    def step(l, s):
        if s <= half:
            serve(l, 0, s)
        if s > lags[l]:
            serve(l, 1, s - lags[l])

    def steps(l, first, end):
        @pl.when(second_core)
        def _():
            for s in range(first, end):
                step(l, s)

        for s in range(first, end):
            if s == lags[l] and l == 0:
                z_first(l, late)

    steps(0, 1, 4)
    steps(0, 4, 5)

    @pl.when(first_core)
    def _():
        x_gather(0)

    @pl.when(second_core)
    def _():
        x_end(0)

    ring_mm(0, 0)
    for s in range(5, half + 1):
        steps(0, s, s + 1)
        ring_mm(0, s - 1)
    steps(0, half + 1, half + 2)
    ring_mm(0, half)

    for l in range(layers):
        final = l == layers - 1
        n = l + 1

        def more(s):
            if not final:
                steps(n, s, s + 1)

        def part(s, sub):
            if not final:

                @pl.when(second_core)
                def _():
                    serve(n, 0, s, (sub,))

        gate(l)
        rest = half + 2
        conv_body(l)
        steps(l, rest, rest + 1)
        if not final:

            @pl.when(second_core)
            def _():
                loaded(n)

            z_first(n, early)
        conv_head(l)
        steps(l, rest + 1, half + lags[l] + 1)
        normalize(l)
        part(1, 0)
        w_wait(l, 1, half)
        give(l, 2, 0)
        give(l, 2, 1)
        give(l, 1, 1)
        part(1, 1)
        pass_on(l, 2, 0, 0)
        pass_on(l, 2, 1, 1)
        give(l, 3, 0)
        pass_on(l, 1, 1, 3)
        part(2, 0)
        give(l, 1, 0)
        pass_on(l, 3, 0, 4)
        give(l, 3, 1)
        part(2, 1)
        give(l, 0, 0)
        give(l, 0, 1)
        part(3, 0)
        pass_on(l, 1, 0, 2, 0)
        pass_on(l, 3, 1, 5, 1)
        part(3, 1)
        if not final:
            z_first(n, late)
        more(4)
        settle(l, 0, final)
        settle(l, 1, final)
        if not final:
            prepare(n)
            x_begin(n)
            stat_start(rstat, n, 0)
            steps(n, 5, half + 1)

            @pl.when(first_core)
            def _():
                x_gather(n)

            @pl.when(second_core)
            def _():
                x_end(n)

            for s in range(7):
                ring_mm(n, s)
            ring_mm(n, half - 1)
            steps(n, half + 1, half + 2)
            ring_mm(n, half)

    for h in range(2):
        pltpu.make_async_copy(result.at[h], out.at[:, h * ch : (h + 1) * ch], out_sem.at[h]).wait()
    for l in range(layers):
        w_drain(l)
        x_drain(l)
        stat_wait(rstat, l, s_send.at[l, 0])
        stat_wait(cstat, l, s_send.at[l, 1])
        halo_copy(l).wait_send()
        part = p_out.at[l]
        pltpu.make_async_copy(part, part, p_send.at[l]).wait()
        part = c_out.at[l]
        pltpu.make_async_copy(part, part, c_send.at[l]).wait()


def solution(mesh):
    sizes = (mesh.shape["grp"], mesh.shape["sp"], mesh.shape["tp"])
    groups, ns, nt = sizes

    def shards(hidden_in, in_gain, w_value, w_gate, conv_taps, norm_gain, norm_shift, w_out):
        layers, rows_w, ch = w_value.shape
        tokens = hidden_in.shape[0]
        vmem = pltpu.VMEM
        dma = pltpu.SemaphoreType.DMA
        half = ns // 2
        scratch = [
            vmem(in_gain.shape, F32),
            vmem((conv_taps.shape[1], layers, ch), F32),
            vmem(norm_gain.shape, F32),
            vmem(norm_shift.shape, F32),
            vmem((2, tokens, ch), BF16),
            vmem(hidden_in.shape, BF16),
            vmem((layers, 2, ns, 3, rows_w, ch), BF16),
            vmem((layers, 2 * nt, tokens, ch), BF16),
            vmem((tokens, 2 * ch), F32),
            vmem((tokens, ch), F32),
            vmem((tokens, ch), F32),
            vmem((tokens, 128), F32),
            vmem((tokens, 128), F32),
            vmem((layers, nt, 8, 128), F32),
            vmem((layers, nt, 2, 8, 128), F32),
            vmem((layers, 32, ch), BF16),
            vmem((layers, 32, ch), BF16),
            vmem((tokens + 32, ch), F32),
            vmem((7, tokens + 24, ch), F32),
            vmem((tokens, ch), F32),
            vmem((tokens, ch), BF16),
            vmem((layers, nt, tokens, ch), BF16),
            vmem((layers, nt, tokens, ch), BF16),
            vmem((layers, 6, tokens, ch), BF16),
            vmem((layers, 6, tokens, ch), BF16),
            dma((layers + 5,)),
            dma((2,)),
            dma((layers,)),
            dma((2, 3, 2, 4)),
            dma((layers,)),
            dma((layers,)),
            dma((layers, 5)),
            dma((layers,)),
            dma((layers,)),
            dma((layers,)),
            dma((13,)),
            dma((layers, 2)),
            dma((2,)),
            dma((layers,)),
            dma((layers,)),
            dma((layers,)),
            dma((nt,)),
            dma((layers,)),
            dma((6,)),
        ]
        a = pl.BlockSpec(memory_space=pl.ANY)
        return pl.pallas_call(
            functools.partial(kernel, sizes),
            out_shape=jax.ShapeDtypeStruct(hidden_in.shape, hidden_in.dtype),
            in_specs=[a] * 8,
            out_specs=a,
            scratch_shapes=scratch,
            name="layers",
            compiler_params=pltpu.CompilerParams(
                collective_id=0, has_side_effects=True, vmem_limit_bytes=60 * 2**20
            ),
        )(hidden_in, in_gain, w_value, w_gate, jnp.transpose(conv_taps, (1, 0, 2)), norm_gain, norm_shift, w_out)

    placed = (
        P(("grp", "sp"), "tp"),
        P(None, "tp"),
        P(None, "sp", "tp"),
        P(None, "sp", "tp"),
        P(None, None, "tp"),
        P(None, "tp"),
        P(None, "tp"),
        P(None, "tp", "sp"),
    )
    return jax.shard_map(
        shards, mesh=mesh, in_specs=placed, out_specs=P(("grp", "sp"), "tp"), check_vma=False
    )
```

```python
import functools

import jax
import jax.numpy as jnp
from jax import lax
from jax.experimental import pallas as pl
from jax.experimental.pallas import tpu as pltpu
from jax.sharding import PartitionSpec as P

MESH = pl.DeviceIdType.MESH
EPS = 1e-06
F32 = jnp.float32
BF16 = jnp.bfloat16
RIGHT, LEFT = 1, -1


def mm(a, b):
    return jnp.dot(a, b, preferred_element_type=F32)


def both(col):
    return jnp.concatenate([col, col], axis=1)


def kernel(
    sizes,
    hidden,
    in_gain_in,
    w_value,
    w_gate,
    taps_in,
    norm_gain_in,
    norm_shift_in,
    w_out,
    out,
    in_gain,
    taps,
    norm_gain,
    norm_shift,
    result,
    start,
    wbuf,
    xg,
    cur,
    acc_v,
    acc_g,
    col_a,
    col_b,
    rstat,
    cstat,
    halo_out,
    halo_in,
    ext,
    shifted,
    conved,
    mixed,
    p_out,
    p_in,
    c_out,
    c_in,
    local_sem,
    out_sem,
    z_send,
    z_recv,
    y_send,
    g_send,
    w_recv,
    m_send,
    m_recv,
    x_send,
    x_recv,
    s_send,
    s_recv,
    h_send,
    h_recv,
    p_send,
    p_recv,
    c_send,
    c_recv,
):
    groups, ns, nt = sizes
    layers = w_value.shape[0]
    rows_w, ch = w_value.shape[1], w_value.shape[2]
    tokens = hidden.shape[0]
    n_taps = taps.shape[0]
    nx = nt // 2
    half = ns // 2
    channels = ch * nt
    features = hidden.shape[1] * nt
    z = lax.axis_index("sp")
    t = lax.axis_index("tp")
    paired = groups % 2 == 0
    x, c = t // 2, lax.rem(t, 2)

    def chip(dx, core):
        return 2 * lax.rem(x + dx + nx, nx) + core

    t_right, t_left, t_opp, t_mate = chip(1, c), chip(-1, c), chip(2, c), 2 * x + (1 - c)

    if paired:
        y = lax.axis_index("grp")
        par = lax.rem(y, 2)
        y_mate = y + 1 - 2 * par
        lone = (96, 80, 80)
    else:
        par, lone = 0, (0, 0, 0)
    ring_rows = tuple(rows_w - rows for rows in lone)

    def rows_at(offset, rows):
        return pl.ds(pl.multiple_of(offset, 16), rows)

    def lone_at(sub):
        return rows_at(par * ring_rows[sub], lone[sub])

    def zc(offset):
        return lax.rem(z + offset + 2 * ns, ns)

    def remote(src, dst, ssem, rsem, **where):
        return pltpu.make_async_remote_copy(
            src_ref=src, dst_ref=dst, send_sem=ssem, recv_sem=rsem, device_id=where, device_id_type=MESH
        )

    split = 96
    pieces = ((0, 0, ring_rows[0]), (1, 0, ring_rows[1]), (2, 0, split), (2, split, ring_rows[2] - split))
    early, late = (0, 1), (2, 3)
    first_core = c == 0
    second_core = c == 1

    def hand_over(l):
        return remote(wbuf.at[l, 0, z], wbuf.at[l, 1, z], m_send.at[l], m_recv.at[l], tp=t_mate)

    def ring_part(l, col, chunk, sub):
        matrix, at, rows = pieces[sub]
        return wbuf.at[l, col, chunk, matrix, rows_at(par * lone[matrix] + at, rows), :]

    def z_copy(l, col, sub, d, s):
        at, way = ring_part(l, col, zc(-d * (s - 1)), sub), 0 if d == RIGHT else 1
        return remote(at, at, z_send.at[l], z_recv.at[col, sub, way, s % 4], sp=zc(d))

    def z_arrival(l, col, sub, d, s):
        at, way = ring_part(l, col, zc(-d * s), sub), 0 if d == RIGHT else 1
        return remote(at, at, z_send.at[l], z_recv.at[col, sub, way, s % 4], sp=zc(d))

    def active(l, sub, d, s):
        if s < half:
            return True
        return s == half and d == (RIGHT, LEFT, RIGHT, LEFT)[sub]

    bulk = half - 2

    def place(kind, d, s):
        if kind == 1:
            return 4
        if s <= bulk:
            return 0
        return 3 if s == half else (1 if d == RIGHT else 2)

    def give_mate(l, kind, sub, d, s):
        chunk = zc(-d * s)
        src, dst = ring_part(l, 1, chunk, sub), ring_part(l, 0, chunk, sub)
        return remote(src, dst, g_send.at[l], w_recv.at[l, place(kind, d, s)], tp=t_mate)

    def y_copy(l, col, matrix, d, s):
        chunk, rows = zc(-d * s), lone_at(matrix)
        src, dst = wbuf.at[l, col, chunk, matrix, rows, :], wbuf.at[l, 0, chunk, matrix, rows, :]
        where = {"grp": y_mate} if col == 0 else {"grp": y_mate, "tp": t_mate}
        return remote(src, dst, y_send.at[l], w_recv.at[l, place(matrix // 2, d, s)], **where)

    def hop_ways(s):
        return (RIGHT, LEFT) if 0 < s < half else (RIGHT,)

    def z_first(l, which):
        @pl.when(second_core)
        def _():
            first = which[0] == 0
            if first and l > 0:
                hand_over(l).wait_recv()
            for col in (0, 1) if first and l == 0 else (1, 0):
                if first and l == 0 and col == 1:
                    hand_over(l).wait_recv()
                for sub in which:
                    for d in (RIGHT, LEFT):
                        z_copy(l, col, sub, d, 1).start()

    def serve(l, kind, s, some=None):
        subs = (early, late)[kind]
        for sub in some or subs:
            for col in (0, 1) if l == 0 and s == 1 else (1, 0):
                for d in (RIGHT, LEFT):
                    if not active(l, sub, d, s):
                        continue
                    z_arrival(l, col, sub, d, s).wait_recv()
                    if active(l, sub, d, s + 1):
                        z_copy(l, col, sub, d, s + 1).start()
                    if col == 1:
                        give_mate(l, kind, sub, d, s).start()
                    if paired and sub != late[0]:
                        y_copy(l, col, pieces[sub][0], d, s).start()

    def take(l, kind, s, matrices, rows):
        if s == 0 or (kind == 0 and s < bulk):
            return
        if kind == 1:
            parts = [(ns - 1, 4)]
        elif s == bulk:
            parts = [(2 * bulk, 0)]
        else:
            parts = [(1, place(0, d, s)) for d in hop_ways(s)]
        for chunks, sem in parts:
            part = wbuf.at[l, 0, pl.ds(0, chunks), pl.ds(0, matrices), pl.ds(0, rows), :]
            pltpu.make_async_copy(part, part, w_recv.at[l, sem]).wait()

    def w_wait(l, kind, s):
        if paired:

            @pl.when(second_core)
            def _():
                take(l, kind, s, 1, lone[2] if kind else lone[0] + lone[1])

        @pl.when(first_core)
        def _():
            take(l, kind, s, 2 - kind, rows_w)

    def w_drain(l):
        def wait(part, sem):
            pltpu.make_async_copy(part, part, sem).wait()

        @pl.when(second_core)
        def _():
            def total(rows):
                subs, rest = rows // rows_w, rows % rows_w
                assert rest == 0
                return wbuf.at[l, :, pl.ds(0, ns - 1), pl.ds(0, subs), :, :]

            sent = total(sum(ring_rows))
            wait(sent, z_send.at[l])
            wait(sent.at[0], g_send.at[l])
            if paired:
                wait(total(sum(lone)), y_send.at[l])

        @pl.when(first_core)
        def _():
            hand_over(l).wait_send()

    def hop_chunks(s):
        if s == 0 or s == half:
            return [zc(s)]
        return [zc(-s), zc(s)]

    from_left, from_right, from_far, from_mate = 0, 4, 8, 12

    def x_copy(l, chunk, where, to):
        at = xg.at[l, chunk]
        return remote(at, at, x_send.at[l], x_recv.at[where], tp=to)

    def x_two(l, owner):
        own = 2 * owner
        part = xg.at[l, pl.ds(own, 2)]
        return remote(part, part, x_send.at[l], x_recv.at[from_mate], tp=t_mate)

    def x_out(l, owner, k):
        a, b = 2 * owner, 2 * owner + 1
        x_copy(l, a, from_left + k, t_right).start()
        x_copy(l, b, from_right + k + 1, t_left).start()
        x_copy(l, b, from_left + k + 1, t_right).start()
        x_copy(l, a, from_right + k, t_left).start()

    def x_begin(l):
        x_two(l, t).start()

        @pl.when(first_core)
        def _():
            x_out(l, t, 0)
            x_two(l, t_mate).wait_recv()
            x_out(l, t_mate, 2)

    def x_share(l, chunk, where):
        x_copy(l, chunk, where, t_mate).wait_recv()
        x_copy(l, chunk, from_mate, t_mate).start()

    def x_gather(l):
        for k in (0, 2):
            core = k // 2
            a, b = 2 * chip(-1, core), 2 * chip(1, core) + 1
            x_copy(l, a, from_left + k, t_mate).wait_recv()
            x_copy(l, a, from_far + k, t_right).start()
            x_copy(l, a, from_mate, t_mate).start()
            x_copy(l, b, from_right + k + 1, t_mate).wait_recv()
            x_copy(l, b, from_far + k + 1, t_left).start()
            x_copy(l, b, from_mate, t_mate).start()
            x_share(l, 2 * chip(-1, core) + 1, from_left + k + 1)
            x_share(l, 2 * chip(1, core), from_right + k)
        for k in (0, 2):
            x_share(l, 2 * chip(2, k // 2), from_far + k)
            x_share(l, 2 * chip(2, k // 2) + 1, from_far + k + 1)

    def x_end(l):
        part = xg.at[l, pl.ds(0, 2 * nt - 2)]
        pltpu.make_async_copy(part, part, x_recv.at[from_mate]).wait()

    def x_drain(l):
        @pl.when(second_core)
        def _():
            x_two(l, t).wait_send()

        @pl.when(first_core)
        def _():
            for count in (2 * nt - 2, 12):
                part = xg.at[l, pl.ds(0, count)]
                pltpu.make_async_copy(part, part, x_send.at[l]).wait()

    def stat_start(buf, l, kind):
        for j in range(1, nt):
            at = buf.at[l, t]
            remote(at, at, s_send.at[l, kind], s_recv.at[kind], tp=lax.rem(t + j, nt)).start()

    def stat_wait(buf, l, sem):
        part = buf.at[l, pl.ds(0, nt - 1)]
        pltpu.make_async_copy(part, part, sem).wait()

    groups_of = tokens // 128

    def to_lanes(column):
        wide = jnp.broadcast_to(column, (tokens, 128)).T[:8]
        row = lax.broadcasted_iota(jnp.int32, (8, 128), 0)
        tile = wide[:, :128]
        for i in range(1, groups_of):
            tile = jnp.where(row == i, wide[:, i * 128 : (i + 1) * 128], tile)
        return tile

    def to_column(tile):
        parts = [jnp.broadcast_to(tile[i : i + 1], (128, 128)).T for i in range(groups_of)]
        return jnp.concatenate(parts, axis=0)

    def prepare(l):
        value = cur[...]
        squares = jnp.sum(value * value, axis=1, keepdims=True)
        rstat[l, t] = to_lanes(squares)
        scaled = (value * in_gain[l : l + 1, :]).astype(BF16)
        xg[l, 2 * t] = scaled[:, : scaled.shape[1] // 2]
        xg[l, 2 * t + 1] = scaled[:, scaled.shape[1] // 2 :]

    def accumulate(l, chunks, first):
        for sub, acc in ((0, acc_v), (1, acc_g)):
            total = None if first else acc[...]
            for chunk in chunks:
                part = mm(xg[l, chunk], wbuf[l, 0, chunk, sub])
                total = part if total is None else total + part
            acc[...] = total

    block = 96

    def over_rows(body):
        def step(i, carry):
            body(pl.multiple_of(i * block, block))
            return carry

        lax.fori_loop(0, tokens // block, step, 0)

    def halo_copy(l):
        return remote(halo_out.at[l], halo_in.at[l], h_send.at[l], h_recv.at[l], sp=zc(1))

    reach = halo_out.shape[1]

    def gate(l):
        stat_wait(rstat, l, s_recv.at[0])
        total = rstat[l, 0]
        for j in range(1, nt):
            total = total + rstat[l, j]
        col_a[...] = to_column(lax.rsqrt(total / features + EPS))

        def body(at):
            rows = pl.ds(at, block)
            scale = both(col_a[rows, :])
            value = acc_v[rows, :] * scale
            gated = value * jax.nn.sigmoid(acc_g[rows, :] * scale)
            ext[pl.ds(pl.multiple_of(at + reach, 32), block), :] = gated.astype(BF16).astype(F32)

        over_rows(body)
        halo_out[l] = ext[tokens : tokens + reach, :].astype(BF16)
        halo_copy(l).start()

    small = 32

    def conv_rows(l, lo, hi):
        offset = reach - (n_taps - 1)

        def step(i, carry):
            at = pl.multiple_of(i * small, small)
            total = jnp.zeros((small, ch), F32)
            for k in range(n_taps):
                a, b = ((k + offset) // 8) * 8, (k + offset) % 8
                rows = pl.ds(pl.multiple_of(at + a, 8), small)
                window = ext[rows, :] if b == 0 else shifted[b - 1, rows, :]
                total = total + taps[k, l : l + 1, :] * window
            conved[pl.ds(at, small), :] = total
            return carry

        lax.fori_loop(lo, hi, step, 0)

    def conv_body(l):
        span = shifted.shape[1]
        for b in range(1, 8):
            shifted[b - 1, reach:, :] = ext[reach + b : span + b, :]
        conv_rows(l, 1, tokens // small)

    def conv_head(l):
        halo_copy(l).wait_recv()
        before = halo_in[l].astype(F32)
        ext[:reach, :] = jnp.where(z > 0, before, jnp.zeros_like(before))
        for b in range(1, 8):
            shifted[b - 1, :reach, :] = ext[b : reach + b, :]
        conv_rows(l, 0, 1)
        value = conved[...]
        sums = jnp.sum(value, axis=1, keepdims=True)
        spread = value - sums / ch
        cstat[l, t, 0] = to_lanes(sums)
        cstat[l, t, 1] = to_lanes(jnp.sum(spread * spread, axis=1, keepdims=True))
        stat_start(cstat, l, 1)

    def normalize(l):
        stat_wait(cstat, l, s_recv.at[1])
        total = cstat[l, 0, 0]
        for j in range(1, nt):
            total = total + cstat[l, j, 0]
        mean = total / channels
        spread = jnp.zeros_like(mean)
        for j in range(nt):
            away = cstat[l, j, 0] / ch - mean
            spread = spread + (cstat[l, j, 1] + ch * (away * away))
        col_a[...] = to_column(mean)
        col_b[...] = to_column(lax.rsqrt(spread / channels + EPS))

        def body(at):
            rows = pl.ds(at, block)
            normed = (conved[rows, :] - both(col_a[rows, :])) * both(col_b[rows, :])
            normed = normed * norm_gain[l : l + 1, :] + norm_shift[l : l + 1, :]
            mixed[rows, :] = (normed / (1.0 + jnp.exp(-normed))).astype(BF16)

        over_rows(body)

    def project(l, dx, core, h):
        return mm(mixed[...], wbuf[l, 0, 2 * chip(dx, core) + h, 2])

    def p_copy(l, q):
        return remote(p_out.at[l, q], p_in.at[l, q], p_send.at[l], p_recv.at[q], tp=t_mate)

    def c_copy(l, slot):
        to = t_right if slot in (0, 2, 3) else t_left
        return remote(c_out.at[l, slot], c_in.at[l, slot], c_send.at[l], c_recv.at[slot], tp=to)

    def give(l, dx, h):
        q = 2 * dx + h
        p_out[l, q] = project(l, dx, 1 - c, h).astype(BF16)
        p_copy(l, q).start()

    def pass_on(l, dx, h, slot, extra=None):
        q = 2 * dx + h
        total = project(l, dx, c, h)
        p_copy(l, q).wait_recv()
        total = total + p_in[l, q].astype(F32)
        if extra is not None:
            c_copy(l, extra).wait_recv()
            total = total + c_in[l, extra].astype(F32)
        c_out[l, slot] = total.astype(BF16)
        c_copy(l, slot).start()

    def settle(l, h, last):
        total = project(l, 0, c, h)
        p_copy(l, h).wait_recv()
        total = total + p_in[l, h].astype(F32)
        for slot in (2 + h, 4 + h):
            c_copy(l, slot).wait_recv()
            total = total + c_in[l, slot].astype(F32)
        cols = slice(h * ch, (h + 1) * ch)
        new = (cur[:, cols] + total).astype(BF16)
        if last:
            result[h] = new
            pltpu.make_async_copy(result.at[h], out.at[:, cols], out_sem.at[h]).start()
        else:
            cur[:, cols] = new.astype(F32)

    barrier = pltpu.get_barrier_semaphore()
    greeted = [{"tp": lax.rem(t + j, nt)} for j in range(1, nt)]
    greeted += [{"sp": zc(1)}, {"sp": zc(-1)}]
    if paired:
        greeted += [{"grp": y_mate}, {"grp": y_mate, "tp": t_mate}]
    for where in greeted:
        pl.semaphore_signal(barrier, inc=1, device_id=where, device_id_type=MESH)

    sources = (w_value, w_gate, w_out)
    loads = [
        pltpu.make_async_copy(src, dst, local_sem.at[layers + i])
        for i, (src, dst) in enumerate(
            (
                (hidden, start),
                (in_gain_in, in_gain),
                (taps_in, taps),
                (norm_gain_in, norm_gain),
                (norm_shift_in, norm_shift),
            )
        )
    ]
    for l in range(layers):
        for sub in range(3):
            pltpu.make_async_copy(sources[sub].at[l], wbuf.at[l, 0, z, sub], local_sem.at[l]).start()
        if l == 0:
            for load in loads:
                load.start()

    def loaded(l):
        part = wbuf.at[l, 0, z]
        pltpu.make_async_copy(part, part, local_sem.at[l]).wait()

    def ring_mm(l, s):
        w_wait(l, 0, s)
        if s == bulk:
            for back in range(1, bulk + 1):
                accumulate(l, hop_chunks(back), False)
        elif s == 0 or s > bulk:
            accumulate(l, hop_chunks(s), s == 0)

    loaded(0)
    pl.semaphore_wait(barrier, len(greeted))

    @pl.when(first_core)
    def _():
        hand_over(0).start()

    z_first(0, early)
    for load in loads:
        load.wait()
    cur[...] = start[...].astype(F32)
    prepare(0)
    x_begin(0)
    stat_start(rstat, 0, 0)

    @pl.when(first_core)
    def _():
        for l in range(1, layers):
            loaded(l)
            hand_over(l).start()

    lags = [3 for l in range(layers)]

    def step(l, s):
        if s <= half:
            serve(l, 0, s)
        if s > lags[l]:
            serve(l, 1, s - lags[l])

    def steps(l, first, end):
        @pl.when(second_core)
        def _():
            for s in range(first, end):
                step(l, s)

        for s in range(first, end):
            if s == lags[l] and l == 0:
                z_first(l, late)

    steps(0, 1, 4)
    steps(0, 4, 5)

    @pl.when(first_core)
    def _():
        x_gather(0)

    @pl.when(second_core)
    def _():
        x_end(0)

    ring_mm(0, 0)
    for s in range(5, half + 1):
        steps(0, s, s + 1)
        ring_mm(0, s - 1)
    steps(0, half + 1, half + 2)
    ring_mm(0, half)

    for l in range(layers):
        final = l == layers - 1
        n = l + 1

        def more(s):
            if not final:
                steps(n, s, s + 1)

        def part(s, sub):
            if not final:

                @pl.when(second_core)
                def _():
                    serve(n, 0, s, (sub,))

        gate(l)
        rest = half + 2
        conv_body(l)
        steps(l, rest, rest + 1)
        if not final:

            @pl.when(second_core)
            def _():
                loaded(n)

            z_first(n, early)
        conv_head(l)
        steps(l, rest + 1, half + lags[l] + 1)
        normalize(l)
        part(1, 0)
        w_wait(l, 1, half)
        give(l, 2, 0)
        give(l, 2, 1)
        give(l, 1, 1)
        part(1, 1)
        pass_on(l, 2, 0, 0)
        pass_on(l, 2, 1, 1)
        give(l, 3, 0)
        pass_on(l, 1, 1, 3)
        part(2, 0)
        give(l, 1, 0)
        pass_on(l, 3, 0, 4)
        give(l, 3, 1)
        part(2, 1)
        give(l, 0, 0)
        give(l, 0, 1)
        part(3, 0)
        pass_on(l, 1, 0, 2, 0)
        pass_on(l, 3, 1, 5, 1)
        part(3, 1)
        if not final:
            z_first(n, late)
        more(4)
        settle(l, 0, final)
        settle(l, 1, final)
        if not final:
            prepare(n)
            x_begin(n)
            stat_start(rstat, n, 0)
            steps(n, 5, half + 1)

            @pl.when(first_core)
            def _():
                x_gather(n)

            @pl.when(second_core)
            def _():
                x_end(n)

            for s in range(half):
                ring_mm(n, s)
            steps(n, half + 1, half + 2)
            ring_mm(n, half)

    for h in range(2):
        pltpu.make_async_copy(result.at[h], out.at[:, h * ch : (h + 1) * ch], out_sem.at[h]).wait()
    for l in range(layers):
        w_drain(l)
        x_drain(l)
        stat_wait(rstat, l, s_send.at[l, 0])
        stat_wait(cstat, l, s_send.at[l, 1])
        halo_copy(l).wait_send()
        part = p_out.at[l]
        pltpu.make_async_copy(part, part, p_send.at[l]).wait()
        part = c_out.at[l]
        pltpu.make_async_copy(part, part, c_send.at[l]).wait()


def solution(mesh):
    sizes = (mesh.shape["grp"], mesh.shape["sp"], mesh.shape["tp"])
    groups, ns, nt = sizes

    def shards(hidden_in, in_gain, w_value, w_gate, conv_taps, norm_gain, norm_shift, w_out):
        layers, rows_w, ch = w_value.shape
        tokens = hidden_in.shape[0]
        vmem = pltpu.VMEM
        dma = pltpu.SemaphoreType.DMA
        half = ns // 2
        scratch = [
            vmem(in_gain.shape, F32),
            vmem((conv_taps.shape[1], layers, ch), F32),
            vmem(norm_gain.shape, F32),
            vmem(norm_shift.shape, F32),
            vmem((2, tokens, ch), BF16),
            vmem(hidden_in.shape, BF16),
            vmem((layers, 2, ns, 3, rows_w, ch), BF16),
            vmem((layers, 2 * nt, tokens, ch), BF16),
            vmem((tokens, 2 * ch), F32),
            vmem((tokens, ch), F32),
            vmem((tokens, ch), F32),
            vmem((tokens, 128), F32),
            vmem((tokens, 128), F32),
            vmem((layers, nt, 8, 128), F32),
            vmem((layers, nt, 2, 8, 128), F32),
            vmem((layers, 32, ch), BF16),
            vmem((layers, 32, ch), BF16),
            vmem((tokens + 32, ch), F32),
            vmem((7, tokens + 24, ch), F32),
            vmem((tokens, ch), F32),
            vmem((tokens, ch), BF16),
            vmem((layers, nt, tokens, ch), BF16),
            vmem((layers, nt, tokens, ch), BF16),
            vmem((layers, 6, tokens, ch), BF16),
            vmem((layers, 6, tokens, ch), BF16),
            dma((layers + 5,)),
            dma((2,)),
            dma((layers,)),
            dma((2, 4, 2, 4)),
            dma((layers,)),
            dma((layers,)),
            dma((layers, 5)),
            dma((layers,)),
            dma((layers,)),
            dma((layers,)),
            dma((13,)),
            dma((layers, 2)),
            dma((2,)),
            dma((layers,)),
            dma((layers,)),
            dma((layers,)),
            dma((nt,)),
            dma((layers,)),
            dma((6,)),
        ]
        a = pl.BlockSpec(memory_space=pl.ANY)
        return pl.pallas_call(
            functools.partial(kernel, sizes),
            out_shape=jax.ShapeDtypeStruct(hidden_in.shape, hidden_in.dtype),
            in_specs=[a] * 8,
            out_specs=a,
            scratch_shapes=scratch,
            name="layers",
            compiler_params=pltpu.CompilerParams(
                collective_id=0, has_side_effects=True, vmem_limit_bytes=60 * 2**20
            ),
        )(hidden_in, in_gain, w_value, w_gate, jnp.transpose(conv_taps, (1, 0, 2)), norm_gain, norm_shift, w_out)

    placed = (
        P(("grp", "sp"), "tp"),
        P(None, "tp"),
        P(None, "sp", "tp"),
        P(None, "sp", "tp"),
        P(None, None, "tp"),
        P(None, "tp"),
        P(None, "tp"),
        P(None, "tp", "sp"),
    )
    return jax.shard_map(
        shards, mesh=mesh, in_specs=placed, out_specs=P(("grp", "sp"), "tp"), check_vma=False
    )
```

```python
import functools

import jax
import jax.numpy as jnp
from jax import lax
from jax.experimental import pallas as pl
from jax.experimental.pallas import tpu as pltpu
from jax.sharding import PartitionSpec as P

MESH = pl.DeviceIdType.MESH
EPS = 1e-06
F32 = jnp.float32
BF16 = jnp.bfloat16
RIGHT, LEFT = 1, -1


def mm(a, b):
    return jnp.dot(a, b, preferred_element_type=F32)


def both(col):
    return jnp.concatenate([col, col], axis=1)


def kernel(
    sizes,
    hidden,
    in_gain_in,
    w_value,
    w_gate,
    taps_in,
    norm_gain_in,
    norm_shift_in,
    w_out,
    out,
    in_gain,
    taps,
    norm_gain,
    norm_shift,
    result,
    start,
    wbuf,
    xg,
    cur,
    acc_v,
    acc_g,
    col_a,
    col_b,
    rstat,
    cstat,
    halo_out,
    halo_in,
    ext,
    shifted,
    conved,
    mixed,
    p_out,
    p_in,
    c_out,
    c_in,
    local_sem,
    out_sem,
    z_send,
    z_recv,
    y_send,
    g_send,
    w_recv,
    m_send,
    m_recv,
    x_send,
    x_recv,
    s_send,
    s_recv,
    h_send,
    h_recv,
    p_send,
    p_recv,
    c_send,
    c_recv,
):
    groups, ns, nt = sizes
    layers = w_value.shape[0]
    rows_w, ch = w_value.shape[1], w_value.shape[2]
    tokens = hidden.shape[0]
    n_taps = taps.shape[0]
    nx = nt // 2
    half = ns // 2
    channels = ch * nt
    features = hidden.shape[1] * nt
    z = lax.axis_index("sp")
    t = lax.axis_index("tp")
    paired = groups % 2 == 0
    x, c = t // 2, lax.rem(t, 2)

    def chip(dx, core):
        return 2 * lax.rem(x + dx + nx, nx) + core

    t_right, t_left, t_opp, t_mate = chip(1, c), chip(-1, c), chip(2, c), 2 * x + (1 - c)

    if paired:
        y = lax.axis_index("grp")
        par = lax.rem(y, 2)
        y_mate = y + 1 - 2 * par
        lone = (96, 80, 80)
    else:
        par, lone = 0, (0, 0, 0)
    ring_rows = tuple(rows_w - rows for rows in lone)

    def rows_at(offset, rows):
        return pl.ds(pl.multiple_of(offset, 16), rows)

    def lone_at(sub):
        return rows_at(par * ring_rows[sub], lone[sub])

    def zc(offset):
        return lax.rem(z + offset + 2 * ns, ns)

    def remote(src, dst, ssem, rsem, **where):
        return pltpu.make_async_remote_copy(
            src_ref=src, dst_ref=dst, send_sem=ssem, recv_sem=rsem, device_id=where, device_id_type=MESH
        )

    split = 96
    pieces = ((0, 0, ring_rows[0]), (1, 0, ring_rows[1]), (2, 0, split), (2, split, ring_rows[2] - split))
    early, late = (0, 1), (2, 3)
    first_core = c == 0
    second_core = c == 1

    def hand_over(l):
        return remote(wbuf.at[l, 0, z], wbuf.at[l, 1, z], m_send.at[l], m_recv.at[l], tp=t_mate)

    def ring_part(l, col, chunk, sub):
        matrix, at, rows = pieces[sub]
        return wbuf.at[l, col, chunk, matrix, rows_at(par * lone[matrix] + at, rows), :]

    def z_copy(l, col, sub, d, s):
        at, way = ring_part(l, col, zc(-d * (s - 1)), sub), 0 if d == RIGHT else 1
        return remote(at, at, z_send.at[l], z_recv.at[col, sub, way, s % 4], sp=zc(d))

    def z_arrival(l, col, sub, d, s):
        at, way = ring_part(l, col, zc(-d * s), sub), 0 if d == RIGHT else 1
        return remote(at, at, z_send.at[l], z_recv.at[col, sub, way, s % 4], sp=zc(d))

    def active(l, sub, d, s):
        if s < half:
            return True
        return s == half and d == (RIGHT, LEFT, RIGHT, LEFT)[sub]

    bulk = half - 2

    def place(kind, d, s):
        if kind == 1:
            return 4
        if s <= bulk:
            return 0
        return 3 if s == half else (1 if d == RIGHT else 2)

    def give_mate(l, kind, sub, d, s):
        chunk = zc(-d * s)
        src, dst = ring_part(l, 1, chunk, sub), ring_part(l, 0, chunk, sub)
        return remote(src, dst, g_send.at[l], w_recv.at[l, place(kind, d, s)], tp=t_mate)

    def y_copy(l, col, matrix, d, s):
        chunk, rows = zc(-d * s), lone_at(matrix)
        src, dst = wbuf.at[l, col, chunk, matrix, rows, :], wbuf.at[l, 0, chunk, matrix, rows, :]
        where = {"grp": y_mate} if col == 0 else {"grp": y_mate, "tp": t_mate}
        return remote(src, dst, y_send.at[l], w_recv.at[l, place(matrix // 2, d, s)], **where)

    def hop_ways(s):
        return (RIGHT, LEFT) if 0 < s < half else (RIGHT,)

    def z_first(l, which):
        @pl.when(second_core)
        def _():
            first = which[0] == 0
            if first and l > 0:
                hand_over(l).wait_recv()
            for col in (0, 1) if first and l == 0 else (1, 0):
                if first and l == 0 and col == 1:
                    hand_over(l).wait_recv()
                for sub in which:
                    for d in (RIGHT, LEFT):
                        z_copy(l, col, sub, d, 1).start()

    def serve(l, kind, s, some=None):
        subs = (early, late)[kind]
        for sub in some or subs:
            for col in (0, 1) if l == 0 and s == 1 else (1, 0):
                for d in (RIGHT, LEFT):
                    if not active(l, sub, d, s):
                        continue
                    z_arrival(l, col, sub, d, s).wait_recv()
                    if active(l, sub, d, s + 1):
                        z_copy(l, col, sub, d, s + 1).start()
                    if col == 1:
                        give_mate(l, kind, sub, d, s).start()
                    if paired and sub != late[0]:
                        y_copy(l, col, pieces[sub][0], d, s).start()

    def take(l, kind, s, matrices, rows):
        if s == 0 or (kind == 0 and s < bulk):
            return
        if kind == 1:
            parts = [(ns - 1, 4)]
        elif s == bulk:
            parts = [(2 * bulk, 0)]
        else:
            parts = [(1, place(0, d, s)) for d in hop_ways(s)]
        for chunks, sem in parts:
            part = wbuf.at[l, 0, pl.ds(0, chunks), pl.ds(0, matrices), pl.ds(0, rows), :]
            pltpu.make_async_copy(part, part, w_recv.at[l, sem]).wait()

    def w_wait(l, kind, s):
        if paired:

            @pl.when(second_core)
            def _():
                take(l, kind, s, 1, lone[2] if kind else lone[0] + lone[1])

        @pl.when(first_core)
        def _():
            take(l, kind, s, 2 - kind, rows_w)

    def w_drain(l):
        def wait(part, sem):
            pltpu.make_async_copy(part, part, sem).wait()

        @pl.when(second_core)
        def _():
            def total(rows):
                subs, rest = rows // rows_w, rows % rows_w
                assert rest == 0
                return wbuf.at[l, :, pl.ds(0, ns - 1), pl.ds(0, subs), :, :]

            sent = total(sum(ring_rows))
            wait(sent, z_send.at[l])
            wait(sent.at[0], g_send.at[l])
            if paired:
                wait(total(sum(lone)), y_send.at[l])

        @pl.when(first_core)
        def _():
            hand_over(l).wait_send()

    def hop_chunks(s):
        if s == 0 or s == half:
            return [zc(s)]
        return [zc(-s), zc(s)]

    from_left, from_right, from_far, from_mate = 0, 4, 8, 12

    def x_copy(l, chunk, where, to):
        at = xg.at[l, chunk]
        return remote(at, at, x_send.at[l], x_recv.at[where], tp=to)

    def x_two(l, owner):
        own = 2 * owner
        part = xg.at[l, pl.ds(own, 2)]
        return remote(part, part, x_send.at[l], x_recv.at[from_mate], tp=t_mate)

    def x_out(l, owner, k):
        a, b = 2 * owner, 2 * owner + 1
        x_copy(l, a, from_left + k, t_right).start()
        x_copy(l, b, from_right + k + 1, t_left).start()
        x_copy(l, b, from_left + k + 1, t_right).start()
        x_copy(l, a, from_right + k, t_left).start()

    def x_begin(l):
        x_two(l, t).start()

        @pl.when(first_core)
        def _():
            x_out(l, t, 0)
            x_two(l, t_mate).wait_recv()
            x_out(l, t_mate, 2)

    def x_share(l, chunk, where):
        x_copy(l, chunk, where, t_mate).wait_recv()
        x_copy(l, chunk, from_mate, t_mate).start()

    def x_gather(l):
        for k in (0, 2):
            core = k // 2
            a, b = 2 * chip(-1, core), 2 * chip(1, core) + 1
            x_copy(l, a, from_left + k, t_mate).wait_recv()
            x_copy(l, a, from_far + k, t_right).start()
            x_copy(l, a, from_mate, t_mate).start()
            x_copy(l, b, from_right + k + 1, t_mate).wait_recv()
            x_copy(l, b, from_far + k + 1, t_left).start()
            x_copy(l, b, from_mate, t_mate).start()
            x_share(l, 2 * chip(-1, core) + 1, from_left + k + 1)
            x_share(l, 2 * chip(1, core), from_right + k)
        for k in (0, 2):
            x_share(l, 2 * chip(2, k // 2), from_far + k)
            x_share(l, 2 * chip(2, k // 2) + 1, from_far + k + 1)

    def x_end(l):
        part = xg.at[l, pl.ds(0, 2 * nt - 2)]
        pltpu.make_async_copy(part, part, x_recv.at[from_mate]).wait()

    def x_drain(l):
        @pl.when(second_core)
        def _():
            x_two(l, t).wait_send()

        @pl.when(first_core)
        def _():
            for count in (2 * nt - 2, 12):
                part = xg.at[l, pl.ds(0, count)]
                pltpu.make_async_copy(part, part, x_send.at[l]).wait()

    def stat_start(buf, l, kind):
        for j in range(1, nt):
            at = buf.at[l, t]
            remote(at, at, s_send.at[l, kind], s_recv.at[kind], tp=lax.rem(t + j, nt)).start()

    def stat_wait(buf, l, sem):
        part = buf.at[l, pl.ds(0, nt - 1)]
        pltpu.make_async_copy(part, part, sem).wait()

    groups_of = tokens // 128

    def to_lanes(column):
        wide = jnp.broadcast_to(column, (tokens, 128)).T[:8]
        row = lax.broadcasted_iota(jnp.int32, (8, 128), 0)
        tile = wide[:, :128]
        for i in range(1, groups_of):
            tile = jnp.where(row == i, wide[:, i * 128 : (i + 1) * 128], tile)
        return tile

    def to_column(tile):
        parts = [jnp.broadcast_to(tile[i : i + 1], (128, 128)).T for i in range(groups_of)]
        return jnp.concatenate(parts, axis=0)

    def prepare(l):
        value = cur[...]
        squares = jnp.sum(value * value, axis=1, keepdims=True)
        rstat[l, t] = to_lanes(squares)
        scaled = (value * in_gain[l : l + 1, :]).astype(BF16)
        xg[l, 2 * t] = scaled[:, : scaled.shape[1] // 2]
        xg[l, 2 * t + 1] = scaled[:, scaled.shape[1] // 2 :]

    def accumulate(l, chunks, first):
        for sub, acc in ((0, acc_v), (1, acc_g)):
            total = None if first else acc[...]
            for chunk in chunks:
                part = mm(xg[l, chunk], wbuf[l, 0, chunk, sub])
                total = part if total is None else total + part
            acc[...] = total

    block = 96

    def over_rows(body):
        def step(i, carry):
            body(pl.multiple_of(i * block, block))
            return carry

        lax.fori_loop(0, tokens // block, step, 0)

    def halo_copy(l):
        return remote(halo_out.at[l], halo_in.at[l], h_send.at[l], h_recv.at[l], sp=zc(1))

    reach = halo_out.shape[1]

    def gate(l):
        stat_wait(rstat, l, s_recv.at[0])
        total = rstat[l, 0]
        for j in range(1, nt):
            total = total + rstat[l, j]
        col_a[...] = to_column(lax.rsqrt(total / features + EPS))

        def body(at):
            rows = pl.ds(at, block)
            scale = both(col_a[rows, :])
            value = acc_v[rows, :] * scale
            gated = value * jax.nn.sigmoid(acc_g[rows, :] * scale)
            ext[pl.ds(pl.multiple_of(at + reach, 32), block), :] = gated.astype(BF16).astype(F32)

        over_rows(body)
        halo_out[l] = ext[tokens : tokens + reach, :].astype(BF16)
        halo_copy(l).start()

    def conv_rows(l, base, small, count):
        offset = reach - (n_taps - 1)

        def step(i, carry):
            at = pl.multiple_of(base + i * small, 8)
            total = jnp.zeros((small, ch), F32)
            for k in range(n_taps):
                a, b = ((k + offset) // 8) * 8, (k + offset) % 8
                rows = pl.ds(pl.multiple_of(at + a, 8), small)
                window = ext[rows, :] if b == 0 else shifted[b - 1, rows, :]
                total = total + taps[k, l : l + 1, :] * window
            conved[pl.ds(at, small), :] = total
            return carry

        lax.fori_loop(0, count, step, 0)

    def conv_body(l):
        span = shifted.shape[1]
        for b in range(1, 8):
            shifted[b - 1, reach:, :] = ext[reach + b : span + b, :]
        conv_rows(l, reach, 88, (tokens - reach) // 88)

    def conv_head(l):
        halo_copy(l).wait_recv()
        before = halo_in[l].astype(F32)
        ext[:reach, :] = jnp.where(z > 0, before, jnp.zeros_like(before))
        for b in range(1, 8):
            shifted[b - 1, :reach, :] = ext[b : reach + b, :]
        conv_rows(l, 0, reach, 1)
        value = conved[...]
        sums = jnp.sum(value, axis=1, keepdims=True)
        spread = value - sums / ch
        cstat[l, t, 0] = to_lanes(sums)
        cstat[l, t, 1] = to_lanes(jnp.sum(spread * spread, axis=1, keepdims=True))
        stat_start(cstat, l, 1)

    def normalize(l):
        stat_wait(cstat, l, s_recv.at[1])
        total = cstat[l, 0, 0]
        for j in range(1, nt):
            total = total + cstat[l, j, 0]
        mean = total / channels
        spread = jnp.zeros_like(mean)
        for j in range(nt):
            away = cstat[l, j, 0] / ch - mean
            spread = spread + (cstat[l, j, 1] + ch * (away * away))
        col_a[...] = to_column(mean)
        col_b[...] = to_column(lax.rsqrt(spread / channels + EPS))

        def body(at):
            rows = pl.ds(at, block)
            normed = (conved[rows, :] - both(col_a[rows, :])) * both(col_b[rows, :])
            normed = normed * norm_gain[l : l + 1, :] + norm_shift[l : l + 1, :]
            mixed[rows, :] = (normed / (1.0 + jnp.exp(-normed))).astype(BF16)

        over_rows(body)

    def project(l, dx, core, h):
        return mm(mixed[...], wbuf[l, 0, 2 * chip(dx, core) + h, 2])

    def p_copy(l, q):
        return remote(p_out.at[l, q], p_in.at[l, q], p_send.at[l], p_recv.at[q], tp=t_mate)

    def c_copy(l, slot):
        to = t_right if slot in (0, 2, 3) else t_left
        return remote(c_out.at[l, slot], c_in.at[l, slot], c_send.at[l], c_recv.at[slot], tp=to)

    def give(l, dx, h):
        q = 2 * dx + h
        p_out[l, q] = project(l, dx, 1 - c, h).astype(BF16)
        p_copy(l, q).start()

    def pass_on(l, dx, h, slot, extra=None):
        q = 2 * dx + h
        total = project(l, dx, c, h)
        p_copy(l, q).wait_recv()
        total = total + p_in[l, q].astype(F32)
        if extra is not None:
            c_copy(l, extra).wait_recv()
            total = total + c_in[l, extra].astype(F32)
        c_out[l, slot] = total.astype(BF16)
        c_copy(l, slot).start()

    def own_part(l, h):
        total = project(l, 0, c, h)
        p_copy(l, h).wait_recv()
        (acc_v, acc_g)[h][...] = total + p_in[l, h].astype(F32)

    def settle(l, h, last):
        total = (acc_v, acc_g)[h][...]
        for slot in (2 + h, 4 + h):
            c_copy(l, slot).wait_recv()
            total = total + c_in[l, slot].astype(F32)
        cols = slice(h * ch, (h + 1) * ch)
        new = (cur[:, cols] + total).astype(BF16)
        if last:
            result[h] = new
            pltpu.make_async_copy(result.at[h], out.at[:, cols], out_sem.at[h]).start()
        else:
            cur[:, cols] = new.astype(F32)

    barrier = pltpu.get_barrier_semaphore()
    greeted = [{"tp": lax.rem(t + j, nt)} for j in range(1, nt)]
    greeted += [{"sp": zc(1)}, {"sp": zc(-1)}]
    if paired:
        greeted += [{"grp": y_mate}, {"grp": y_mate, "tp": t_mate}]
    for where in greeted:
        pl.semaphore_signal(barrier, inc=1, device_id=where, device_id_type=MESH)

    sources = (w_value, w_gate, w_out)
    loads = [
        pltpu.make_async_copy(src, dst, local_sem.at[layers + i])
        for i, (src, dst) in enumerate(
            (
                (hidden, start),
                (in_gain_in, in_gain),
                (taps_in, taps),
                (norm_gain_in, norm_gain),
                (norm_shift_in, norm_shift),
            )
        )
    ]
    for l in range(layers):
        for sub in range(3):
            pltpu.make_async_copy(sources[sub].at[l], wbuf.at[l, 0, z, sub], local_sem.at[l]).start()
        if l == 0:
            for load in loads:
                load.start()

    def loaded(l):
        part = wbuf.at[l, 0, z]
        pltpu.make_async_copy(part, part, local_sem.at[l]).wait()

    def ring_mm(l, s):
        w_wait(l, 0, s)
        if s == bulk:
            for back in range(1, bulk + 1):
                accumulate(l, hop_chunks(back), False)
        elif s == 0 or s > bulk:
            accumulate(l, hop_chunks(s), s == 0)

    loaded(0)
    pl.semaphore_wait(barrier, len(greeted))

    @pl.when(first_core)
    def _():
        hand_over(0).start()

    z_first(0, early)
    for load in loads:
        load.wait()
    cur[...] = start[...].astype(F32)
    prepare(0)
    x_begin(0)
    stat_start(rstat, 0, 0)

    @pl.when(first_core)
    def _():
        for l in range(1, layers):
            loaded(l)
            hand_over(l).start()

    lags = [3 for l in range(layers)]

    def step(l, s):
        if s <= half:
            serve(l, 0, s)
        if s > lags[l]:
            serve(l, 1, s - lags[l])

    def steps(l, first, end):
        @pl.when(second_core)
        def _():
            for s in range(first, end):
                step(l, s)

        for s in range(first, end):
            if s == lags[l] and l == 0:
                z_first(l, late)

    steps(0, 1, 4)
    steps(0, 4, 5)

    @pl.when(first_core)
    def _():
        x_gather(0)

    @pl.when(second_core)
    def _():
        x_end(0)

    ring_mm(0, 0)
    for s in range(5, half + 1):
        steps(0, s, s + 1)
        ring_mm(0, s - 1)
    steps(0, half + 1, half + 2)
    ring_mm(0, half)

    for l in range(layers):
        final = l == layers - 1
        n = l + 1

        def more(s):
            if not final:
                steps(n, s, s + 1)

        def part(s, sub):
            if not final:

                @pl.when(second_core)
                def _():
                    serve(n, 0, s, (sub,))

        gate(l)
        rest = half + 2
        conv_body(l)
        steps(l, rest, rest + 1)
        if not final:

            @pl.when(second_core)
            def _():
                loaded(n)

            z_first(n, early)
        conv_head(l)
        steps(l, rest + 1, half + lags[l] + 1)
        normalize(l)
        part(1, 0)
        w_wait(l, 1, half)
        give(l, 2, 0)
        give(l, 2, 1)
        give(l, 1, 1)
        part(1, 1)
        pass_on(l, 2, 0, 0)
        pass_on(l, 2, 1, 1)
        give(l, 3, 0)
        pass_on(l, 1, 1, 3)
        part(2, 0)
        give(l, 1, 0)
        pass_on(l, 3, 0, 4)
        give(l, 3, 1)
        part(2, 1)
        give(l, 0, 0)
        give(l, 0, 1)
        part(3, 0)
        pass_on(l, 1, 0, 2, 0)
        pass_on(l, 3, 1, 5, 1)
        part(3, 1)
        if not final:
            z_first(n, late)
        own_part(l, 0)
        own_part(l, 1)
        more(4)
        settle(l, 0, final)
        settle(l, 1, final)
        if not final:
            prepare(n)
            x_begin(n)
            stat_start(rstat, n, 0)
            steps(n, 5, half + 1)

            @pl.when(first_core)
            def _():
                x_gather(n)

            @pl.when(second_core)
            def _():
                x_end(n)

            for s in range(half):
                ring_mm(n, s)
            steps(n, half + 1, half + 2)
            ring_mm(n, half)

    for h in range(2):
        pltpu.make_async_copy(result.at[h], out.at[:, h * ch : (h + 1) * ch], out_sem.at[h]).wait()
    for l in range(layers):
        w_drain(l)
        x_drain(l)
        stat_wait(rstat, l, s_send.at[l, 0])
        stat_wait(cstat, l, s_send.at[l, 1])
        halo_copy(l).wait_send()
        part = p_out.at[l]
        pltpu.make_async_copy(part, part, p_send.at[l]).wait()
        part = c_out.at[l]
        pltpu.make_async_copy(part, part, c_send.at[l]).wait()


def solution(mesh):
    sizes = (mesh.shape["grp"], mesh.shape["sp"], mesh.shape["tp"])
    groups, ns, nt = sizes

    def shards(hidden_in, in_gain, w_value, w_gate, conv_taps, norm_gain, norm_shift, w_out):
        layers, rows_w, ch = w_value.shape
        tokens = hidden_in.shape[0]
        vmem = pltpu.VMEM
        dma = pltpu.SemaphoreType.DMA
        half = ns // 2
        scratch = [
            vmem(in_gain.shape, F32),
            vmem((conv_taps.shape[1], layers, ch), F32),
            vmem(norm_gain.shape, F32),
            vmem(norm_shift.shape, F32),
            vmem((2, tokens, ch), BF16),
            vmem(hidden_in.shape, BF16),
            vmem((layers, 2, ns, 3, rows_w, ch), BF16),
            vmem((layers, 2 * nt, tokens, ch), BF16),
            vmem((tokens, 2 * ch), F32),
            vmem((tokens, ch), F32),
            vmem((tokens, ch), F32),
            vmem((tokens, 128), F32),
            vmem((tokens, 128), F32),
            vmem((layers, nt, 8, 128), F32),
            vmem((layers, nt, 2, 8, 128), F32),
            vmem((layers, 32, ch), BF16),
            vmem((layers, 32, ch), BF16),
            vmem((tokens + 32, ch), F32),
            vmem((7, tokens + 24, ch), F32),
            vmem((tokens, ch), F32),
            vmem((tokens, ch), BF16),
            vmem((layers, nt, tokens, ch), BF16),
            vmem((layers, nt, tokens, ch), BF16),
            vmem((layers, 6, tokens, ch), BF16),
            vmem((layers, 6, tokens, ch), BF16),
            dma((layers + 5,)),
            dma((2,)),
            dma((layers,)),
            dma((2, 4, 2, 4)),
            dma((layers,)),
            dma((layers,)),
            dma((layers, 5)),
            dma((layers,)),
            dma((layers,)),
            dma((layers,)),
            dma((13,)),
            dma((layers, 2)),
            dma((2,)),
            dma((layers,)),
            dma((layers,)),
            dma((layers,)),
            dma((nt,)),
            dma((layers,)),
            dma((6,)),
        ]
        a, b = pl.BlockSpec(memory_space=pltpu.HBM), pl.BlockSpec(memory_space=pl.ANY)
        taps = jnp.transpose(conv_taps, (1, 0, 2))
        operands = (hidden_in, in_gain, w_value, w_gate, taps, norm_gain, norm_shift, w_out)
        return pl.pallas_call(
            functools.partial(kernel, sizes),
            out_shape=jax.ShapeDtypeStruct(hidden_in.shape, hidden_in.dtype),
            in_specs=[a] * 8,
            out_specs=b,
            scratch_shapes=scratch,
            name="layers",
            compiler_params=pltpu.CompilerParams(
                collective_id=0, has_side_effects=True, vmem_limit_bytes=52 * 2**20
            ),
        )(*(pltpu.with_memory_space_constraint(operand, pltpu.HBM) for operand in operands))

    placed = (
        P(("grp", "sp"), "tp"),
        P(None, "tp"),
        P(None, "sp", "tp"),
        P(None, "sp", "tp"),
        P(None, None, "tp"),
        P(None, "tp"),
        P(None, "tp"),
        P(None, "tp", "sp"),
    )
    return jax.shard_map(
        shards, mesh=mesh, in_specs=placed, out_specs=P(("grp", "sp"), "tp"), check_vma=False
    )
```
